256 devices in a mesh: ep: 64 (over z, x, core), tp: 4 (over y).
Axes of the slice: x: 4, y: 4, z: 8, core: 2. Of those that a mesh axis runs over, the one named last changes fastest.
Arguments:
- tokens: bfloat16 [1024, 2048], P('ep'), may hold values from -6 to 6
- norm1_gain: float32 [2048], replicated, may hold values from 0.1 to 1.9
- query_weight: bfloat16 [2048, 512], P(None, 'tp'), may hold values from -0.125 to 0.125
- key_weight: bfloat16 [2048, 256], P(None, 'tp'), may hold values from -0.125 to 0.125
- value_weight: bfloat16 [2048, 256], P(None, 'tp'), may hold values from -0.125 to 0.125
- forget_weight: bfloat16 [2048, 8], P(None, 'tp'), may hold values from -0.125 to 0.125
- forget_bias: float32 [8], P('tp'), may hold values from 0.5 to 4
- out_weight: bfloat16 [512, 2048], P('tp'), may hold values from -0.25 to 0.25
- kv_cache: bfloat16 [1024, 1024, 4, 128], P('ep', None, 'tp'), may hold values from -6 to 6
- log_gates: float32 [1024, 8, 1024], P('ep', 'tp'), may hold values from -1024 to 0, as said below
- lengths: int32 [1024], P('ep'), may hold values from 64 to 1024
- norm2_gain: float32 [2048], replicated, may hold values from 0.1 to 1.9
- routing: int32 [1024, 4], P('ep'), may hold values from 0 to 63, all different within a row; in each aligned block of 16 rows (0 to 15, 16 to 31, ...) at most 3 rows name the same one
- route_weight: float32 [1024, 4], P('ep'), may hold values from 0.1 to 0.6
- expert_gate: bfloat16 [64, 2048, 2048], P('ep', None, 'tp'), may hold values from -0.25 to 0.25
- expert_up: bfloat16 [64, 2048, 2048], P('ep', None, 'tp'), may hold values from -0.25 to 0.25
- expert_down: bfloat16 [64, 2048, 2048], P('ep', 'tp'), may hold values from -0.0625 to 0.0625
- dense_gate: bfloat16 [2048, 4096], P(None, 'ep'), may hold values from -0.25 to 0.25
- dense_up: bfloat16 [2048, 4096], P(None, 'ep'), may hold values from -0.25 to 0.25
- dense_down: bfloat16 [4096, 2048], P('ep'), may hold values from -0.09375 to 0.09375
- dense_mix: float32 [2048], replicated, may hold values from -0.125 to 0.125
Outputs:
- layer_out: bfloat16 [1024, 2048], P(('ep', 'tp'))
The draws below stay inside these ranges and needn't reach their ends.
Inputs may be any that keep to these rules, and one draw needn't show every extreme that they name: `log_gates`: Non-increasing along the positions. `routing`: each row names 4 different experts. Among the rows of one index of ep (aligned blocks of 16 rows) no expert is named by more than 3 rows, and in every draw some expert is named by exactly 3 rows of some block.
All inputs are finite; a program needn't handle non-finite values.
Results may differ from the reference program's by a relative error of at most 0.011.
Values may be sent and summed in bfloat16 or wider, within the bound.
A program may use at most 128 MiB of HBM per device.

```python
import math
from functools import partial
import jax
import jax.numpy as jnp
import numpy as np
from jax import lax

D = 2048
QUERY_HEADS = 8
KV_HEADS = 4
HEAD_DIM = 64
EXP_FF = 2048
DENSE_FF = 4096
TOP = 4
SEQ_GRP = 16
CACHE_POSITIONS = 1024
BATCH_SEQUENCES = 1024
EXPERTS = 64
CAP = 3
N_EP = 64


def draw_log_gates(key, part):
    random_subkeys = jax.random.split(jax.random.fold_in(key, 7), 6)
    slow_share = 0.5
    is_slow = jax.random.uniform(random_subkeys[0], (1, QUERY_HEADS, 1)) < slow_share
    slow_rate = jnp.exp(jax.random.uniform(random_subkeys[1], (1, QUERY_HEADS, 1), minval=jnp.log(0.3), maxval=jnp.log(1.5))) / CACHE_POSITIONS
    fast_rate = 1.0 / jnp.exp(jax.random.uniform(random_subkeys[2], (1, QUERY_HEADS, 1), minval=jnp.log(30.0), maxval=jnp.log(100.0)))
    per_seq = jnp.exp(jax.random.uniform(random_subkeys[3], (BATCH_SEQUENCES, 1, 1), minval=jnp.log(0.5), maxval=jnp.log(2.0)))
    roughness = jax.random.uniform(random_subkeys[4], (BATCH_SEQUENCES, QUERY_HEADS, CACHE_POSITIONS), minval=0.25, maxval=1.75)
    logarithm_increments = -jnp.where(is_slow, slow_rate, fast_rate) * per_seq * roughness
    spike_sample = jax.random.uniform(random_subkeys[5], (BATCH_SEQUENCES, QUERY_HEADS, CACHE_POSITIONS))
    spike_events = spike_sample < 3.0 / CACHE_POSITIONS
    spike_penalty = jnp.log(1.0 - (0.2 + 0.3 * jnp.clip(spike_sample * CACHE_POSITIONS / 3.0, 0.0, 1.0)))
    logarithm_increments = jnp.where(spike_events, logarithm_increments + spike_penalty, logarithm_increments)
    return jnp.cumsum(logarithm_increments, axis=2).astype(jnp.float32)


def touch_ends(entries, rng, low, largest):
    spot = [jax.random.randint(jax.random.fold_in(rng, axis), (), 0, length) for axis, length in enumerate(entries.shape)]
    widest = entries.shape.index(max(entries.shape))
    next_to = spot[:widest] + [(spot[widest] + 1) % entries.shape[widest]] + spot[widest + 1:]
    return entries.at[tuple(spot)].set(low).at[tuple(next_to)].set(largest)


def levels(key, extent, cuts, smallest, high):
    level = 1.0
    for axis_at, shards_of in cuts:
        heights = jax.random.uniform(jax.random.fold_in(jax.random.fold_in(key, 6), axis_at), (shards_of,), jnp.float32, smallest / len(cuts), high / len(cuts))
        level = level * jnp.repeat(jnp.exp(heights), extent[axis_at] // shards_of).reshape((-1,) + (1,) * (len(extent) - 1 - axis_at))
    return level


def shared_out(rng, own, number, rows, count, top, bound, lean):
    order = jax.random.permutation(rng, count)
    heavy_load, usual = portions_of(count, rows * top, bound, lean, True), portions_of(count, rows * top, bound, lean, False)
    places = jnp.arange(count)

    def named(tallies, offset_by):
        used = int((tallies > 0).sum())
        fixed = max(1, used // 4)
        shifted = fixed + (places - fixed + offset_by * (used - fixed)) % max(1, count - fixed)
        return jnp.zeros((count,), jnp.int32).at[order[jnp.where(places < fixed, places, shifted)]].set(jnp.asarray(tallies, jnp.int32))

    tallies = jnp.where(number % 4 == 0, named(heavy_load, number // 4), named(usual, number - number // 4 - 1))
    mixed = jax.random.permutation(jax.random.fold_in(own, 3), count)
    giver, receiver = mixed[0:count // 2 * 2:2], mixed[1:count // 2 * 2:2]
    slack = jnp.minimum(tallies[giver] - 1, bound - tallies[receiver]) // 2
    slack = jnp.where((giver == order[0]) | (receiver == order[0]) | (tallies[receiver] == 0), 0, jnp.maximum(slack, 0))
    shifted = jax.random.randint(jax.random.fold_in(own, 4), (count // 2,), 0, 1 << 20) % (slack + 1)
    tallies = tallies.at[giver].add(-shifted).at[receiver].add(shifted)
    members = jnp.searchsorted(jnp.cumsum(tallies), jnp.arange(rows * top), side="right").astype(jnp.int32)
    listing = members.reshape(top, rows).T
    listing = listing[jax.random.permutation(jax.random.fold_in(own, 1), rows)]
    offset_by = jax.random.randint(jax.random.fold_in(own, 2), (rows, 1), 0, top)
    return jnp.take_along_axis(listing, (jnp.arange(top)[None, :] + offset_by) % top, axis=1)


def portions_of(count, total, limit, lean, full):
    portions = [(1 << 20) // math.isqrt(rank ** lean) + 1 for rank in range(1, count + 1)]
    largest = limit if full else min(limit, max(-(-total // count), total * portions[0] // sum(portions)))
    least = 1 if total - largest >= count - 1 else 0
    holding, surplus = [largest] + [least] * (count - 1), total - largest - least * (count - 1)
    while surplus > 0:
        movable = [i for i in range(1, count) if holding[i] < largest] or [i for i in range(1, count) if holding[i] < limit]
        mass, left = sum([portions[i] for i in movable]), surplus
        for i in movable:
            more = min(limit - holding[i], max(1, left * portions[i] // mass), surplus)
            holding[i] = holding[i] + more
            surplus = surplus - more
    return np.array(holding)


def bell_draw(stream_key, extent, deviation, limit, cuts=(), kind=jnp.bfloat16):
    result = jax.random.normal(stream_key, extent, jnp.float32) * deviation
    if len(cuts) > 0:
        result = levels(stream_key, extent, cuts, -0.22, 0.18) * result
    return jnp.clip(result, min=-limit, max=limit).astype(kind)


def setup_inputs(seed: int = 0) -> dict:
    keys = jax.random.split(jax.random.key(seed), 22)
    tokens = bell_draw(keys[0], (BATCH_SEQUENCES, D), 1.0, 6.0, ((0, 64),))
    norm1_gain = jnp.clip(1.0 + 0.18 * jax.random.normal(keys[1], (D,), jnp.float32), 0.1, 1.9)
    query_weight = bell_draw(keys[2], (D, QUERY_HEADS * HEAD_DIM), D ** -0.5, 0.125, ((1, 4),))
    key_weight = bell_draw(keys[3], (D, KV_HEADS * HEAD_DIM), D ** -0.5, 0.125, ((1, 4),))
    value_weight = bell_draw(keys[4], (D, KV_HEADS * HEAD_DIM), D ** -0.5, 0.125, ((1, 4),))
    forget_weight = bell_draw(keys[5], (D, QUERY_HEADS), D ** -0.5, 0.125, ((1, 4),))
    forget_bias = jnp.clip(0.5 + 3.5 * jax.random.uniform(keys[6], (QUERY_HEADS,), jnp.float32) ** levels(keys[6], (QUERY_HEADS,), ((0, 4),), -0.2, 0.2), 0.5, 4.0)
    out_weight = bell_draw(keys[7], (QUERY_HEADS * HEAD_DIM, D), (QUERY_HEADS * HEAD_DIM) ** -0.5, 0.25, ((0, 4),))
    kv_cache = bell_draw(keys[8], (BATCH_SEQUENCES, CACHE_POSITIONS, KV_HEADS, 2 * HEAD_DIM), 1.0, 6.0, ((0, 64), (2, 4)))
    log_gates = draw_log_gates(jax.random.fold_in(keys[21], 71), 0)
    lengths = touch_ends(jax.random.randint(keys[10], (BATCH_SEQUENCES,), CACHE_POSITIONS // 16, CACHE_POSITIONS + 1), jax.random.fold_in(keys[10], 1), CACHE_POSITIONS // 16, CACHE_POSITIONS).astype(jnp.int32)
    norm2_gain = jnp.clip(1.0 + 0.18 * jax.random.normal(keys[11], (D,), jnp.float32), 0.1, 1.9)
    routing_keys = jax.random.split(jax.random.fold_in(keys[12], 1), BATCH_SEQUENCES // SEQ_GRP)
    routing_turns = jax.random.permutation(jax.random.fold_in(keys[12], 3), BATCH_SEQUENCES // SEQ_GRP)
    routing = jax.vmap(lambda own, number: shared_out(jax.random.fold_in(keys[12], 2), own, number, SEQ_GRP, EXPERTS, TOP, CAP, 2))(routing_keys, routing_turns).reshape((BATCH_SEQUENCES, TOP))
    route_weight = jnp.clip(0.1 + 0.5 * jax.random.uniform(keys[13], (BATCH_SEQUENCES, TOP), jnp.float32) ** levels(keys[13], (BATCH_SEQUENCES, TOP), ((0, 64),), -0.2, 0.2), 0.1, 0.6)
    expert_gate = bell_draw(keys[14], (EXPERTS, D, EXP_FF), (D // 4) ** -0.5, 0.25, ((0, 64), (2, 4)))
    expert_up = bell_draw(keys[15], (EXPERTS, D, EXP_FF), (D // 4) ** -0.5, 0.25, ((0, 64), (2, 4)))
    expert_down = bell_draw(keys[16], (EXPERTS, EXP_FF, D), (4 * EXP_FF) ** -0.5, 0.0625, ((0, 64), (1, 4)))
    dense_gate = bell_draw(keys[17], (D, DENSE_FF), (D // 4) ** -0.5, 0.25, ((1, 64),))
    dense_up = bell_draw(keys[18], (D, DENSE_FF), (D // 4) ** -0.5, 0.25, ((1, 64),))
    dense_down = bell_draw(keys[19], (DENSE_FF, D), DENSE_FF ** -0.5, 0.09375, ((0, 64),))
    dense_mix = bell_draw(keys[20], (D,), D ** -0.5, 0.125, (), jnp.float32)
    return dict(tokens=tokens, norm1_gain=norm1_gain, query_weight=query_weight, key_weight=key_weight, value_weight=value_weight, forget_weight=forget_weight, forget_bias=forget_bias, out_weight=out_weight, kv_cache=kv_cache, log_gates=log_gates, lengths=lengths, norm2_gain=norm2_gain, routing=routing, route_weight=route_weight, expert_gate=expert_gate, expert_up=expert_up, expert_down=expert_down, dense_gate=dense_gate, dense_up=dense_up, dense_down=dense_down, dense_mix=dense_mix)


EPS = 1e-05
LIMIT = 7.0
ALPHA = 1.702

def clamped_unit(gate_pre, up_pre):
    capped = jnp.minimum(gate_pre, LIMIT)
    return capped * jax.nn.sigmoid(ALPHA * capped) * (jnp.clip(up_pre, -LIMIT, LIMIT) + 1.0)

def rms_scaled(values, gain_vec):
    return values * lax.rsqrt(lax.optimization_barrier(jnp.mean(values * values, axis=-1, keepdims=True)) + EPS) * gain_vec

def slot_tables(routes, experts, capacity):
    flat_ids = routes.reshape(-1)
    onehot = (flat_ids[:, None] == jnp.arange(experts, dtype=jnp.int32)[None, :]).astype(jnp.int32)
    earlier = jnp.cumsum(onehot, axis=0, dtype=jnp.int32) - onehot
    slot_ids = lax.optimization_barrier(jnp.sum(earlier * onehot, axis=1, dtype=jnp.int32))
    matches = onehot[:, :, None] * (slot_ids[:, None, None] == jnp.arange(capacity, dtype=jnp.int32)[None, None, :]).astype(jnp.int32)
    owners = jnp.arange(flat_ids.shape[0], dtype=jnp.int32) // routes.shape[1]
    source = lax.optimization_barrier(jnp.sum(matches * owners[:, None, None], axis=0, dtype=jnp.int32))
    return (slot_ids, source)

def attend_group(block_args):
    queries, key_new, value_new, gate_new, cache, gates, seq_lens = block_args
    seq_count, cache_len, kv_heads, doubled = cache.shape
    head_dim = doubled // 2
    head_count = gate_new.shape[1]
    per_kv = head_count // kv_heads
    score_scale = head_dim ** (-0.5)
    query_f32 = queries.astype(jnp.float32).reshape(seq_count, kv_heads, per_kv, head_dim)
    keys_f32 = cache[..., :head_dim].astype(jnp.float32)
    vals_f32 = cache[..., head_dim:].astype(jnp.float32)
    scores = jnp.einsum('skgd,slkd->skgl', query_f32, keys_f32) * score_scale
    last_index = jnp.broadcast_to((seq_lens - 1).astype(jnp.int32)[:, None, None], (seq_count, head_count, 1))
    last_gate = jnp.take_along_axis(gates, last_index, axis=2)
    gate_bias = (last_gate - gates + gate_new[:, :, None]).reshape(seq_count, kv_heads, per_kv, cache_len)
    live_mask = (jnp.arange(cache_len, dtype=jnp.int32)[None, :] < seq_lens[:, None])[:, None, None, :]
    cached = jnp.where(live_mask, jnp.exp(scores + gate_bias), 0.0)
    own_keys = key_new.astype(jnp.float32).reshape(seq_count, kv_heads, head_dim)
    own_exp = jnp.exp(jnp.einsum('skgd,skd->skg', query_f32, own_keys) * score_scale)
    denominator = lax.optimization_barrier(jnp.sum(cached, axis=-1)) + own_exp
    weight_cache = lax.optimization_barrier((cached / denominator[..., None]).astype(jnp.bfloat16))
    weight_own = lax.optimization_barrier((own_exp / denominator).astype(jnp.bfloat16))
    attended = jnp.einsum('skgl,slkd->skgd', weight_cache.astype(jnp.float32), vals_f32)
    own_vals = value_new.astype(jnp.float32).reshape(seq_count, kv_heads, 1, head_dim)
    attended = attended + weight_own.astype(jnp.float32)[..., None] * own_vals
    return attended.astype(jnp.bfloat16).reshape(seq_count, head_count * head_dim)

def reference(tokens, norm1_gain, query_weight, key_weight, value_weight, forget_weight, forget_bias, out_weight, kv_cache, log_gates, lengths, norm2_gain, routing, route_weight, expert_gate, expert_up, expert_down, dense_gate, dense_up, dense_down, dense_mix):
    normed = rms_scaled(tokens.astype(jnp.float32), norm1_gain).astype(jnp.bfloat16)
    queries = jnp.dot(normed, query_weight, preferred_element_type=jnp.float32).astype(jnp.bfloat16)
    key_new = jnp.dot(normed, key_weight, preferred_element_type=jnp.float32).astype(jnp.bfloat16)
    value_new = jnp.dot(normed, value_weight, preferred_element_type=jnp.float32).astype(jnp.bfloat16)
    gate_new = jax.nn.log_sigmoid(jnp.dot(normed, forget_weight, preferred_element_type=jnp.float32) + forget_bias)
    operands = [queries, key_new, value_new, gate_new, kv_cache, log_gates, lengths]
    grouped = tuple((operand.reshape((N_EP, SEQ_GRP) + operand.shape[1:]) for operand in operands))
    attended = lax.map(attend_group, grouped).reshape(BATCH_SEQUENCES, QUERY_HEADS * HEAD_DIM)
    attn_out = jnp.dot(attended, out_weight, preferred_element_type=jnp.float32).astype(jnp.bfloat16)
    residual = tokens.astype(jnp.float32) + attn_out.astype(jnp.float32)
    hidden_in = lax.optimization_barrier(rms_scaled(residual, norm2_gain).astype(jnp.bfloat16))
    slot_ids, source = jax.vmap(partial(slot_tables, experts=EXPERTS, capacity=CAP))(routing.reshape(N_EP, SEQ_GRP, TOP))
    group_base = (jnp.arange(N_EP, dtype=jnp.int32) * SEQ_GRP)[:, None, None]
    rows_index = jnp.transpose(source + group_base, (1, 0, 2)).reshape(EXPERTS, N_EP * CAP)

    def run_expert(block_args):
        index_row, gate_w, up_w, down_w = block_args
        picked = hidden_in[index_row]
        gate_pre = jnp.dot(picked, gate_w, preferred_element_type=jnp.float32)
        up_pre = jnp.dot(picked, up_w, preferred_element_type=jnp.float32)
        activation = clamped_unit(gate_pre, up_pre).astype(jnp.bfloat16)
        return jnp.dot(activation, down_w, preferred_element_type=jnp.float32).astype(jnp.bfloat16)
    expert_out = lax.map(run_expert, (rows_index, expert_gate, expert_up, expert_down))
    block_of_row = (jnp.arange(BATCH_SEQUENCES, dtype=jnp.int32) // SEQ_GRP)[:, None]
    flat_index = (routing * N_EP + block_of_row) * CAP + slot_ids.reshape(BATCH_SEQUENCES, TOP)
    picked_out = expert_out.reshape(EXPERTS * N_EP * CAP, D)[flat_index.reshape(-1)].reshape(BATCH_SEQUENCES, TOP, D)
    moe_val = lax.optimization_barrier(jnp.sum(route_weight[..., None] * picked_out.astype(jnp.float32), axis=1))
    dense_gate_pre = jnp.dot(hidden_in, dense_gate, preferred_element_type=jnp.float32)
    dense_up_pre = jnp.dot(hidden_in, dense_up, preferred_element_type=jnp.float32)
    dense_act = clamped_unit(dense_gate_pre, dense_up_pre).astype(jnp.bfloat16)
    dense_val = jnp.dot(dense_act, dense_down, preferred_element_type=jnp.float32)
    mix_gate = jax.nn.sigmoid(jnp.dot(hidden_in.astype(jnp.float32), dense_mix, precision=lax.Precision.HIGHEST))
    return (residual + moe_val + mix_gate[:, None] * dense_val).astype(jnp.bfloat16)
```

```python
import functools

import jax
import jax.numpy as jnp
import numpy as np
from jax import lax
from jax.experimental import pallas as pl
from jax.experimental.pallas import tpu as pltpu
from jax.sharding import PartitionSpec as P

EPS = 1e-05
LIMIT = 7.0
ALPHA = 1.702
NZ, NX, NC = 8, 4, 2
CAP = 3
META = 128
MESH = pl.DeviceIdType.MESH


def clamped_unit(gate_pre, up_pre):
    capped = jnp.minimum(gate_pre, LIMIT)
    return capped * jax.nn.sigmoid(ALPHA * capped) * (jnp.clip(up_pre, -LIMIT, LIMIT) + 1.0)


def rms_scaled(values, gain_vec):
    return values * lax.rsqrt(jnp.mean(values * values, axis=-1, keepdims=True) + EPS) * gain_vec


def remote(src, dst, send_sem, recv_sem, **device):
    return pltpu.make_async_remote_copy(
        src_ref=src,
        dst_ref=dst,
        send_sem=send_sem,
        recv_sem=recv_sem,
        device_id=device,
        device_id_type=MESH,
    )


def layer_kernel(
    top,
    part,
    tok,
    gain2,
    meta,
    dmix,
    gs,
    cb,
    own_xc,
    eg_hbm,
    eu_hbm,
    ed_hbm,
    wlo_hbm,
    whi_hbm,
    dd_hbm,
    out,
    h_all,
    eg,
    eu,
    ed,
    wlo,
    whi,
    dd,
    s1buf,
    yb,
    resid,
    pick,
    xs,
    ysend,
    yrecv,
    rown,
    zs,
    zr,
    zf,
    asend,
    arecv,
    cs,
    c32,
    cr,
    fs,
    fr,
    ldsem,
    s1s,
    s1r,
    s2s,
    s2r,
    xss,
    xrs,
    rss,
    rrs,
    lss,
    lrs,
    dcs,
    dcr,
    dds,
    ddr,
    yss,
    yrs,
    zss,
    zrs,
    ass,
    ars,
    css,
    crs,
    fss,
    frs,
):
    ny, rows4, d_model = part.shape
    seq = meta.shape[0]
    nblk = NC * NZ * NX
    n_rows = nblk * seq
    fq = d_model // ny
    nxc = NX * NC
    zrows = CAP * nxc
    f32, bf16 = jnp.float32, jnp.bfloat16
    ep = lax.axis_index("ep")
    t = lax.axis_index("tp")
    z = ep // nxc
    x = (ep // NC) % NX
    c = ep % NC

    def ep_at(zi, xi, ci):
        return (zi * NX + xi) * NC + ci

    def blk(ci, zi, xi):
        return (ci * NZ + zi) * NX + xi

    def yp(d):
        return lax.rem(t + d + ny, ny)

    def zp(d):
        return lax.rem(z + d + NZ, NZ)

    def xp(d):
        return lax.rem(x + d + NX, NX)

    def cp(d):
        return lax.rem(c + d, NC)

    xc_rel = [(dx, dc) for dc in range(NC) for dx in range(NX) if dx or dc]

    barrier = pltpu.get_barrier_semaphore()
    for d in range(1, ny):
        pl.semaphore_signal(barrier, inc=1, device_id={"tp": yp(d)}, device_id_type=MESH)
    for dx, dc in xc_rel:
        pl.semaphore_signal(
            barrier, inc=1, device_id={"ep": ep_at(z, xp(dx), cp(dc))}, device_id_type=MESH
        )
    for d in range(1, NZ):
        pl.semaphore_signal(
            barrier, inc=1, device_id={"ep": ep_at(zp(d), x, c)}, device_id_type=MESH
        )

    loads = [
        pltpu.make_async_copy(src, dst, ldsem.at[i])
        for i, (src, dst) in enumerate(
            [
                (eg_hbm, eg),
                (eu_hbm, eu),
                (ed_hbm, ed),
                (wlo_hbm, wlo),
                (whi_hbm, whi),
                (dd_hbm.at[:, pl.ds(pl.multiple_of(t * fq, fq), fq)], dd.at[z, 0]),
            ]
        )
    ]
    for load in loads:
        load.start()
    pl.semaphore_wait(barrier, (ny - 1) + len(xc_rel) + (NZ - 1))

    sent = []

    def go(copy):
        copy.start()
        sent.append(copy)

    firsts = [
        remote(part.at[yp(d)], s1buf.at[d - 1], s1s.at[d - 1], s1r.at[d - 1], tp=yp(d))
        for d in range(1, ny)
    ]
    for copy in firsts:
        go(copy)
    total = part[t]
    for d, copy in enumerate(firsts):
        copy.wait_recv()
        total = total + s1buf[d]
    res = tok[t].astype(f32) + total.astype(bf16).astype(f32)
    resid[...] = res
    yb[t] = rms_scaled(res, gain2[...]).astype(bf16)
    for d in range(1, ny):
        go(remote(yb.at[t], yb.at[t], s2s.at[d - 1], s2r.at[d - 1], tp=yp(d)))
    for d in range(1, ny):
        there = yb.at[yp(-d)]
        remote(there, there, s2s.at[d - 1], s2r.at[d - 1], tp=yp(-d)).wait_recv()
    mine = h_all.at[blk(c, z, x)]
    mine[:, :d_model] = jnp.concatenate([yb[j].astype(f32) for j in range(ny)], axis=0).astype(bf16)
    mine[:, d_model:] = meta[...]

    for d in range(1, NX):
        go(remote(mine, mine, xss.at[d - 1], xrs.at[d - 1], ep=ep_at(z, xp(d), c)))

    half = (NX + 1) // 2
    last = NZ // 2

    def takes(direction, step, q):
        if step < last:
            return True
        return q < half if direction > 0 else q >= half

    def pass_on(direction, step, q):
        if step > last or not takes(direction, step, q):
            return
        block = h_all.at[blk(c, zp(-direction * (step - 1)), xp(-q))]
        ss, rs = (rss, rrs) if direction > 0 else (lss, lrs)
        go(
            remote(
                block, block, ss.at[step - 1, q], rs.at[step - 1, q], ep=ep_at(zp(direction), x, c)
            )
        )

    def across(rel, q):
        block = h_all.at[blk(c, zp(rel), xp(-q))]
        i = rel % NZ
        go(remote(block, block, dcs.at[i, q], dcr.at[i, q], ep=ep_at(z, x, cp(1))))

    for q in range(NX):
        if q:
            block = h_all.at[blk(c, z, xp(-q))]
            remote(block, block, xss.at[q - 1], xrs.at[q - 1], ep=ep_at(z, xp(-q), c)).wait_recv()
        pass_on(1, 1, q)
        pass_on(-1, 1, q)
        across(0, q)
    for step in range(1, last + 1):
        for q in range(NX):
            for direction in (1, -1):
                if not takes(direction, step, q):
                    continue
                rs, ss = (rrs, rss) if direction > 0 else (lrs, lss)
                block = h_all.at[blk(c, zp(-direction * step), xp(-q))]
                remote(
                    block,
                    block,
                    ss.at[step - 1, q],
                    rs.at[step - 1, q],
                    ep=ep_at(zp(-direction), x, c),
                ).wait_recv()
                pass_on(direction, step + 1, q)
                across(-direction * step, q)
    for rel in range(NZ):
        for q in range(NX):
            block = h_all.at[blk(cp(1), zp(rel), xp(-q))]
            remote(block, block, dcs.at[rel, q], dcr.at[rel, q], ep=ep_at(z, x, cp(1))).wait_recv()

    for load in loads:
        load.wait()
    for d in range(1, NZ):
        go(
            remote(
                dd.at[z, 0], dd.at[z, 0], dds.at[d - 1], ddr.at[d - 1], ep=ep_at(zp(d), x, c)
            )
        )

    codes = h_all[:, :, d_model:].reshape(n_rows, META)
    lead = lax.broadcasted_iota(jnp.int32, (8, META), 0)
    lane = lax.broadcasted_iota(jnp.int32, (8, META), 1)
    unit = jnp.where(lead == lane, 1.0, 0.0).astype(bf16)
    code_rows = lax.dot_general(
        unit, codes, (((1,), (1,)), ((), ())), preferred_element_type=f32
    )
    slot = jnp.full((1, n_rows), -1.0, f32)
    base = (ep * 4).astype(f32)
    for k in range(top):
        j = code_rows[k : k + 1] - base
        slot = jnp.where((j >= 0.0) & (j <= CAP - 1.0), gs[0:1] + j * nxc, slot)
    slots = NZ * zrows
    order = lax.broadcasted_iota(jnp.int32, (slots, n_rows), 0).astype(f32)
    pick[...] = jnp.where(order == slot, 1.0, 0.0).astype(bf16)
    step_n = min(512, d_model)
    for n in range(0, d_model, step_n):
        xs[:, n : n + step_n] = jnp.dot(
            pick[...],
            h_all[:, :, n : n + step_n].reshape(n_rows, step_n),
            preferred_element_type=f32,
        ).astype(bf16)
    act = clamped_unit(
        jnp.dot(xs[...], eg[...], preferred_element_type=f32),
        jnp.dot(xs[...], eu[...], preferred_element_type=f32),
    ).astype(bf16)

    z_order = sorted(range(NZ), key=lambda d: -min(d, NZ - d))
    y_order = sorted(range(1, ny), key=lambda d: -min(d, ny - d))

    def block_result(peer):
        return jnp.dot(
            act, ed[:, pl.ds(pl.multiple_of(peer * fq, fq), fq)], preferred_element_type=f32
        )

    for d in y_order:
        made = block_result(yp(d))
        for zi in range(NZ):
            ysend[d - 1, zi] = made[zi * zrows : (zi + 1) * zrows].astype(bf16)
        for dz in z_order:
            zi = zp(dz)
            go(
                remote(
                    ysend.at[d - 1, zi],
                    yrecv.at[d - 1, zi],
                    yss.at[d - 1, dz],
                    yrs.at[d - 1, dz],
                    tp=yp(d),
                )
            )
    made = block_result(t)
    for zi in range(NZ):
        rown[zi] = made[zi * zrows : (zi + 1) * zrows]

    per_z = NX * seq
    two_units = wlo.shape[1] // 2
    for zi in range(NZ):
        low = h_all[blk(0, zi, 0) : blk(0, zi, 0) + NX, :, :d_model].reshape(per_z, d_model)
        high = h_all[blk(1, zi, 0) : blk(1, zi, 0) + NX, :, :d_model].reshape(per_z, d_model)
        pre = jnp.dot(low, wlo[...], preferred_element_type=f32) + jnp.dot(
            high, whi[...], preferred_element_type=f32
        )
        asend[zi] = clamped_unit(pre[:, :two_units], pre[:, two_units:]).astype(bf16)
    for dz in z_order[:-1]:
        go(
            remote(
                asend.at[zp(dz)],
                arecv.at[z],
                ass.at[dz - 1],
                ars.at[dz - 1],
                ep=ep_at(zp(dz), x, c),
            )
        )
    arecv[z] = asend[z]

    own_rows = [h_all[pl.ds(blk(ci, z, 0), NX)].reshape(per_z, d_model + META) for ci in range(NC)]
    own_meta = jnp.concatenate([r[:, d_model:].astype(f32) for r in own_rows], axis=0)
    mix = jnp.concatenate(
        [
            jnp.sum(r[:, :d_model].astype(f32) * dmix[...], axis=-1, keepdims=True)
            for r in own_rows
        ],
        axis=0,
    )
    mix = jax.nn.sigmoid(mix)
    targets = cb[0:1] + (4 * (x * NC + c)).astype(f32)
    spread = jnp.zeros((NC * per_z, slots), f32)
    for k in range(top):
        weight = (
            own_meta[:, top + k : top + k + 1]
            + own_meta[:, 2 * top + k : 2 * top + k + 1]
            + own_meta[:, 3 * top + k : 3 * top + k + 1]
        )
        spread = spread + jnp.where(own_meta[:, k : k + 1] == targets, weight, 0.0)
    spread = spread * own_xc[...]
    spread_high = spread.astype(bf16)
    spread_low = (spread - spread_high.astype(f32)).astype(bf16)

    for dz in z_order:
        zi = zp(dz)
        summed = rown[zi]
        for d in range(1, ny):
            there = yrecv.at[d - 1, zi]
            remote(
                ysend.at[d - 1, zi], there, yss.at[d - 1, dz], yrs.at[d - 1, dz], tp=yp(-d)
            ).wait_recv()
            summed = summed + there[...].astype(f32)
        if dz:
            zs[zi] = summed.astype(bf16)
            go(
                remote(
                    zs.at[zi], zr.at[z], zss.at[dz - 1], zrs.at[dz - 1], ep=ep_at(zi, x, c)
                )
            )
        else:
            zr[z] = summed.astype(bf16)

    for d in range(1, NZ):
        there = dd.at[zp(-d), 0]
        remote(there, there, dds.at[d - 1], ddr.at[d - 1], ep=ep_at(zp(-d), x, c)).wait_recv()
    for d in range(1, NZ):
        there = arecv.at[zp(-d)]
        remote(there, there, ass.at[d - 1], ars.at[d - 1], ep=ep_at(zp(-d), x, c)).wait_recv()
    units = two_units // 2
    first = lax.broadcasted_iota(jnp.int32, (per_z, two_units), 1) < units
    dense = jnp.zeros((NC * per_z, fq), f32)
    for j in range(NZ):
        dd[j, 1] = dd[j, 0]
        got = arecv[j].astype(f32)
        both = jnp.concatenate(
            [jnp.where(first, got, 0.0), jnp.where(first, 0.0, got)], axis=0
        ).astype(bf16)
        dense = dense + jnp.dot(
            both, dd[j].reshape(two_units, fq), preferred_element_type=f32
        )
    for d in range(1, NZ):
        there = zr.at[zp(-d)]
        remote(there, there, zss.at[d - 1], zrs.at[d - 1], ep=ep_at(zp(-d), x, c)).wait_recv()
    for j in range(NZ):
        zf[j * zrows : (j + 1) * zrows] = zr[j].astype(f32)
    results = zf[...].astype(bf16)
    mixed = (
        jnp.dot(spread_high, results, preferred_element_type=f32)
        + jnp.dot(spread_low, results, preferred_element_type=f32)
        + mix * dense
    )
    c32[...] = mixed.reshape(nxc, seq, fq)
    cs[...] = mixed.astype(bf16).reshape(nxc, seq, fq)

    def xc_at(xi, ci):
        return ci * NX + xi

    for i, (dx, dc) in enumerate(xc_rel):
        xi, ci = xp(dx), cp(dc)
        go(remote(cs.at[xc_at(xi, ci)], cr.at[i], css.at[i], crs.at[i], ep=ep_at(z, xi, ci)))
    moe = c32[xc_at(x, c)]
    for i, (dx, dc) in enumerate(xc_rel):
        remote(cs.at[0], cr.at[i], css.at[i], crs.at[i], ep=ep_at(z, xp(-dx), cp(dc))).wait_recv()
        moe = moe + cr[i].astype(f32)

    for j in range(ny):
        fs[j] = moe[j * rows4 : (j + 1) * rows4]
    for d in range(1, ny):
        go(remote(fs.at[yp(d)], fr.at[t], fss.at[d - 1], frs.at[d - 1], tp=yp(d)))
    fr[t] = fs[t]
    for d in range(1, ny):
        there = fr.at[yp(-d)]
        remote(fs.at[0], there, fss.at[d - 1], frs.at[d - 1], tp=yp(-d)).wait_recv()
    for j in range(ny):
        cols = slice(j * fq, (j + 1) * fq)
        out[:, cols] = (resid[:, cols] + fr[j]).astype(bf16)
    for copy in sent:
        copy.wait_send()


def after_attention(
    partial_out,
    tokens,
    norm2_gain,
    routing,
    route_weight,
    expert_gate,
    expert_up,
    expert_down,
    dense_gate,
    dense_up,
    dense_down,
    dense_mix,
):
    seq, d_model = tokens.shape
    top = routing.shape[1]
    ny = lax.axis_size("tp")
    rows4 = seq // ny
    ff = expert_gate.shape[2]
    units = dense_gate.shape[1]
    fq = d_model // ny
    nxc = NX * NC
    nblk = NC * NZ * NX
    n_rows = nblk * seq
    zrows = CAP * nxc
    slots = NZ * zrows
    f32, bf16 = jnp.float32, jnp.bfloat16

    same = routing[:, :, None, None] == routing[None, None, :, :]
    before = (jnp.arange(seq)[None, :] < jnp.arange(seq)[:, None])[:, None, :, None]
    rank = jnp.sum((same & before).astype(jnp.int32), axis=(2, 3))
    high = lax.reduce_precision(route_weight, 8, 7)
    mid = lax.reduce_precision(route_weight - high, 8, 7)
    low = route_weight - high - mid
    meta = jnp.concatenate([(routing * 4 + rank).astype(f32), high, mid, low], axis=1)
    meta = jnp.pad(meta, ((0, 0), (0, META - 4 * top))).astype(bf16)

    b = np.arange(n_rows) // seq
    bx, bz, bc = b % NX, (b // NX) % NZ, b // (NX * NZ)
    gs = np.broadcast_to((bz * zrows + bx * NC + bc).astype(np.float32), (8, n_rows))
    s = np.arange(slots)
    cb = np.broadcast_to((4 * nxc * (s // zrows) + (s % zrows) // nxc).astype(np.float32), (8, slots))
    r = np.arange(NC * NX * seq) // seq
    own_xc = ((r % NX) * NC + r // NX)[:, None] == (s % nxc)[None, :]

    none = jnp.zeros((d_model, units), bf16)
    wlo = jnp.concatenate([dense_gate, none, dense_up, none], axis=1)
    whi = jnp.concatenate([none, dense_gate, none, dense_up], axis=1)

    dma = pltpu.SemaphoreType.DMA
    vm = pltpu.VMEM
    width = d_model + META
    last = NZ // 2
    scratch = [
        vm((nblk, seq, width), bf16),
        vm((d_model, ff), bf16),
        vm((d_model, ff), bf16),
        vm((ff, d_model), bf16),
        vm((d_model, 4 * units), bf16),
        vm((d_model, 4 * units), bf16),
        vm((NZ, 2, units, fq), bf16),
        vm((ny - 1, rows4, d_model), f32),
        vm((ny, rows4, d_model), bf16),
        vm((rows4, d_model), f32),
        vm((slots, n_rows), bf16),
        vm((slots, d_model), bf16),
        vm((ny - 1, NZ, zrows, fq), bf16),
        vm((ny - 1, NZ, zrows, fq), bf16),
        vm((NZ, zrows, fq), f32),
        vm((NZ, zrows, fq), bf16),
        vm((NZ, zrows, fq), bf16),
        vm((slots, fq), f32),
        vm((NZ, NX * seq, 2 * units), bf16),
        vm((NZ, NX * seq, 2 * units), bf16),
        vm((nxc, seq, fq), bf16),
        vm((nxc, seq, fq), f32),
        vm((nxc - 1, seq, fq), bf16),
        vm((ny, rows4, fq), f32),
        vm((ny, rows4, fq), f32),
        dma((6,)),
    ]
    scratch += [dma((ny - 1,))] * 4
    scratch += [dma((max(NX - 1, 1),))] * 2
    scratch += [dma((last, NX))] * 4
    scratch += [dma((NZ, NX))] * 2
    scratch += [dma((NZ - 1,))] * 2
    scratch += [dma((ny - 1, NZ))] * 2
    scratch += [dma((NZ - 1,))] * 4
    scratch += [dma((nxc - 1,))] * 2
    scratch += [dma((ny - 1,))] * 2
    in_vmem = pl.BlockSpec(memory_space=pltpu.VMEM)
    in_hbm = pl.BlockSpec(memory_space=pl.ANY)
    return pl.pallas_call(
        functools.partial(layer_kernel, top),
        out_shape=jax.ShapeDtypeStruct((rows4, d_model), bf16),
        in_specs=[in_vmem] * 8 + [in_hbm] * 6,
        out_specs=in_vmem,
        scratch_shapes=scratch,
        compiler_params=pltpu.CompilerParams(
            collective_id=0, has_side_effects=True, vmem_limit_bytes=60 * 1024 * 1024
        ),
        name="layer",
    )(
        partial_out.reshape(ny, rows4, d_model),
        tokens.reshape(ny, rows4, d_model),
        norm2_gain.reshape(1, d_model),
        meta,
        dense_mix.reshape(1, d_model),
        jnp.asarray(gs),
        jnp.asarray(cb),
        jnp.asarray(own_xc.astype(np.float32)),
        expert_gate[0],
        expert_up[0],
        expert_down[0],
        wlo,
        whi,
        dense_down,
    )


def on_device(
    tokens,
    norm1_gain,
    query_weight,
    key_weight,
    value_weight,
    forget_weight,
    forget_bias,
    out_weight,
    kv_cache,
    log_gates,
    lengths,
    norm2_gain,
    routing,
    route_weight,
    expert_gate,
    expert_up,
    expert_down,
    dense_gate,
    dense_up,
    dense_down,
    dense_mix,
):
    seq_count, model_width = tokens.shape
    local_heads = forget_bias.shape[0]
    kv_local = kv_cache.shape[2]
    head_dim = kv_cache.shape[3] // 2
    per_kv = local_heads // kv_local
    cache_len = kv_cache.shape[1]
    score_scale = head_dim ** (-0.5)
    normed = rms_scaled(tokens.astype(jnp.float32), norm1_gain).astype(jnp.bfloat16)
    queries = jnp.dot(normed, query_weight, preferred_element_type=jnp.float32).astype(jnp.bfloat16)
    queries = queries.reshape(seq_count, kv_local, per_kv, head_dim)
    key_new = jnp.dot(normed, key_weight, preferred_element_type=jnp.float32).astype(jnp.bfloat16)
    key_new = key_new.reshape(seq_count, kv_local, head_dim)
    value_new = jnp.dot(normed, value_weight, preferred_element_type=jnp.float32).astype(
        jnp.bfloat16
    )
    value_new = value_new.reshape(seq_count, kv_local, head_dim)
    gate_new = jax.nn.log_sigmoid(
        jnp.dot(normed, forget_weight, preferred_element_type=jnp.float32) + forget_bias
    )
    scores = (
        jnp.einsum(
            "skgd,slkd->skgl", queries, kv_cache[..., :head_dim], preferred_element_type=jnp.float32
        )
        * score_scale
    )
    last_index = jnp.broadcast_to((lengths - 1)[:, None, None], (seq_count, local_heads, 1))
    last_gate = jnp.take_along_axis(log_gates, last_index, axis=2)
    gate_bias = (last_gate - log_gates + gate_new[:, :, None]).reshape(
        seq_count, kv_local, per_kv, cache_len
    )
    live_mask = (jnp.arange(cache_len, dtype=jnp.int32)[None, :] < lengths[:, None])[
        :, None, None, :
    ]
    cached = jnp.where(live_mask, jnp.exp(scores + gate_bias), 0.0)
    own_exp = jnp.exp(
        jnp.einsum("skgd,skd->skg", queries, key_new, preferred_element_type=jnp.float32)
        * score_scale
    )
    denominator = jnp.sum(cached, axis=-1) + own_exp
    weight_cache = (cached / denominator[..., None]).astype(jnp.bfloat16)
    weight_own = (own_exp / denominator).astype(jnp.bfloat16)
    attended = jnp.einsum(
        "skgl,slkd->skgd",
        weight_cache,
        kv_cache[..., head_dim:],
        preferred_element_type=jnp.float32,
    )
    attended = (
        attended
        + weight_own.astype(jnp.float32)[..., None] * value_new.astype(jnp.float32)[:, :, None, :]
    )
    attended = attended.astype(jnp.bfloat16).reshape(seq_count, local_heads * head_dim)
    partial_out = jnp.dot(attended, out_weight, preferred_element_type=jnp.float32)
    return after_attention(
        partial_out,
        tokens,
        norm2_gain,
        routing,
        route_weight,
        expert_gate,
        expert_up,
        expert_down,
        dense_gate,
        dense_up,
        dense_down,
        dense_mix,
    )


def solution(mesh):
    return jax.shard_map(
        on_device,
        mesh=mesh,
        in_specs=(
            P("ep", None),
            P(),
            P(None, "tp"),
            P(None, "tp"),
            P(None, "tp"),
            P(None, "tp"),
            P("tp"),
            P("tp", None),
            P("ep", None, "tp", None),
            P("ep", "tp", None),
            P("ep"),
            P(),
            P("ep", None),
            P("ep", None),
            P("ep", None, "tp"),
            P("ep", None, "tp"),
            P("ep", "tp", None),
            P(None, "ep"),
            P(None, "ep"),
            P("ep", None),
            P(),
        ),
        out_specs=P(("ep", "tp"), None),
        check_vma=False,
    )
```

```python
import functools

import jax
import jax.numpy as jnp
from jax import lax
from jax.experimental import pallas as pl
from jax.experimental.pallas import tpu as pltpu
from jax.sharding import PartitionSpec as P

EPS = 1e-05
LIMIT = 7.0
ALPHA = 1.702
NZ, NX, NC = 8, 4, 2
CAP = 3
META = 128
MESH = pl.DeviceIdType.MESH


def clamped_unit(gate_pre, up_pre):
    capped = jnp.minimum(gate_pre, LIMIT)
    return capped * jax.nn.sigmoid(ALPHA * capped) * (jnp.clip(up_pre, -LIMIT, LIMIT) + 1.0)


def rms_scaled(values, gain_vec):
    return values * lax.rsqrt(jnp.mean(values * values, axis=-1, keepdims=True) + EPS) * gain_vec


def remote(src, dst, send_sem, recv_sem, **device):
    return pltpu.make_async_remote_copy(
        src_ref=src,
        dst_ref=dst,
        send_sem=send_sem,
        recv_sem=recv_sem,
        device_id=device,
        device_id_type=MESH,
    )


IN_NAMES = (
    "tok",
    "gain1",
    "gain2",
    "dmix",
    "wq",
    "wkt",
    "wvt",
    "fwt",
    "fbias",
    "lengths",
    "gates",
    "routing",
    "weight",
    "wout",
    "kv",
    "eg_hbm",
    "eu_hbm",
    "ed_hbm",
    "dgt",
    "dut",
    "dd_hbm",
)
VMEM_INPUTS = 13


class Refs:
    pass


def layer_kernel(names, top, *refs):
    r = Refs()
    for name, ref in zip(names, refs, strict=True):
        setattr(r, name, ref)
    seq, d_model = r.tok.shape
    ny = r.part.shape[0]
    rows4 = seq // ny
    nblk = NC * NZ * NX
    fq = d_model // ny
    nxc = NX * NC
    zrows = CAP * nxc
    slots = NZ * zrows
    per_z = NX * seq
    both_z = NC * per_z
    f32, bf16 = jnp.float32, jnp.bfloat16
    h_all = r.h_all
    ep = lax.axis_index("ep")
    t = lax.axis_index("tp")
    z = ep // nxc
    x = (ep // NC) % NX
    c = ep % NC

    def ep_at(zi, xi, ci):
        return (zi * NX + xi) * NC + ci

    def blk(ci, zi, xi):
        return (ci * NZ + zi) * NX + xi

    def yp(d):
        return lax.rem(t + d + ny, ny)

    def zp(d):
        return lax.rem(z + d + NZ, NZ)

    def xp(d):
        return lax.rem(x + d + NX, NX)

    def cp(d):
        return lax.rem(c + d, NC)

    def iota(shape, dim):
        return lax.broadcasted_iota(jnp.int32, shape, dim)

    def dot_nt(a, b):
        return lax.dot_general(a, b, (((1,), (1,)), ((), ())), preferred_element_type=f32)

    def dot(a, b):
        return jnp.dot(a, b, preferred_element_type=f32)

    y_order = sorted(range(1, ny), key=lambda d: -min(d, ny - d))

    barrier = pltpu.get_barrier_semaphore()
    plane = [(dt, dx, dc) for dt in range(ny) for dc in range(NC) for dx in range(NX)][1:]
    for dt, dx, dc in plane:
        pl.semaphore_signal(
            barrier,
            inc=1,
            device_id={"ep": ep_at(z, xp(dx), cp(dc)), "tp": yp(dt)},
            device_id_type=MESH,
        )
    for d in range(1, NZ):
        pl.semaphore_signal(
            barrier, inc=1, device_id={"ep": ep_at(zp(d), x, c)}, device_id_type=MESH
        )

    units = r.dgt.shape[0]
    kv_groups = 4
    per_group = seq // kv_groups
    kv_loads = [
        pltpu.make_async_copy(
            r.kv.at[pl.ds(i * per_group, per_group)],
            r.kvbuf.at[pl.ds(i * per_group, per_group)],
            r.kvsem.at[i],
        )
        for i in range(kv_groups)
    ]
    late = [
        (r.dd_hbm.at[:, pl.ds(pl.multiple_of(t * fq, fq), fq)], r.dd.at[NZ - 1]),
        (r.wout, r.wo),
        (r.dgt, r.wgu.at[pl.ds(0, units)]),
        (r.dut, r.wgu.at[pl.ds(units, units)]),
        (r.eg_hbm, r.eg),
        (r.eu_hbm, r.eu),
        (r.ed_hbm, r.ed),
    ]
    late = [pltpu.make_async_copy(src, dst, r.ldsem.at[i]) for i, (src, dst) in enumerate(late)]
    for load in kv_loads + late:
        load.start()

    sent = {}

    def go(key, src, dst, recv_sem, **device):
        remote(src, dst, getattr(r, key), recv_sem, **device).start()
        sent[key] = sent.get(key, 0) + 1

    def arrived(ref, recv_sem):
        remote(ref, ref, r.s_dd, recv_sem, ep=ep, tp=t).wait_recv()

    tok = r.tok[...].astype(f32)
    normed = rms_scaled(tok, r.gain1[...])
    normed = normed.astype(bf16)
    hd = r.wkt.shape[0]
    cache_len = r.kv.shape[1]
    scale = hd ** (-0.5)
    q = dot(normed, r.wq[...]).astype(bf16).astype(f32)
    r.wkv[:hd] = r.wkt[...]
    r.wkv[hd:] = r.wvt[...]
    kv_new = dot_nt(normed, r.wkv[...]).astype(bf16).astype(f32)
    low_lanes = iota((seq, 2 * hd), 1) < hd
    q_heads = [jnp.where(low_lanes, q, 0.0), jnp.where(low_lanes, pltpu.roll(q, hd, 1), 0.0)]
    wide = normed.astype(f32)
    pairs = 2 * seq
    of_pair = iota((pairs, seq), 0) == 2 * iota((pairs, seq), 1)
    of_pair1 = iota((pairs, seq), 0) == 2 * iota((pairs, seq), 1) + 1
    eye = jnp.where(iota((seq, seq), 0) == iota((seq, seq), 1), 1.0, 0.0)

    def to_pairs(first, second):
        rows = [jnp.sum(eye * v, axis=0, keepdims=True) for v in (first, second)]
        return jnp.sum(
            jnp.where(of_pair, rows[0], jnp.where(of_pair1, rows[1], 0.0)), axis=1, keepdims=True
        )

    of_heads = [jnp.where(m, 1.0, 0.0).astype(bf16) for m in (of_pair, of_pair1)]
    q_pairs = sum(dot(of_heads[h], q_heads[h].astype(bf16)) for h in range(2))
    kv_pairs = dot(of_heads[0] + of_heads[1], kv_new.astype(bf16))
    gate_new, own_exp = [], []
    for h in range(2):
        pre = jnp.sum(wide * r.fwt[h : h + 1, :].astype(f32), axis=-1, keepdims=True)
        pre = pre + r.fbias[0, h]
        gate_new.append(jnp.minimum(pre, 0.0) - jnp.log(1.0 + jnp.exp(-jnp.abs(pre))))
        own_exp.append(jnp.exp(jnp.sum(q_heads[h] * kv_new, axis=-1, keepdims=True) * scale))
    gate_new = to_pairs(*gate_new)
    own_exp = to_pairs(*own_exp)

    rt = r.routing[...].astype(f32)
    wt = r.weight[...]
    earlier = iota((seq, seq), 1) < iota((seq, seq), 0)
    lane = iota((seq, META), 1)
    meta = jnp.zeros((seq, META), f32)

    def column(row):
        return jnp.sum(eye * row, axis=-1, keepdims=True)

    for k in range(top):
        chosen = column(rt[k : k + 1])
        same = jnp.zeros((seq, seq), f32)
        for other in range(top):
            same = same + jnp.where((chosen == rt[other : other + 1]) & earlier, 1.0, 0.0)
        rank = jnp.sum(same, axis=-1, keepdims=True)
        value = column(wt[k : k + 1])
        high = value.astype(bf16).astype(f32)
        mid = (value - high).astype(bf16).astype(f32)
        parts = (4.0 * chosen + rank, high, mid, value - high - mid)
        for i, v in enumerate(parts):
            meta = jnp.where(lane == i * top + k, v, meta)

    position = iota((8, cache_len), 1)
    row_pair = iota((8, 1), 0) // 2
    row_pair_wide = iota((8, 2 * hd), 0) // 2

    for g in range(kv_groups):
        kv_loads[g].wait()
        if g == kv_groups // 2:
            pl.semaphore_wait(barrier, len(plane) + (NZ - 1))
            late[0].wait()
            for d in range(1, NZ):
                go("s_dd", r.dd.at[NZ - 1], r.dd.at[d - 1], r.ddr, ep=ep_at(zp(d), x, c))
        at = slice(8 * g, 8 * g + 8)
        queries = q_pairs[at]
        scores = jnp.zeros((8, cache_len), f32)
        length = jnp.zeros((8, 1), jnp.int32)
        for i in range(4):
            only = jnp.where(row_pair_wide == i, queries, 0.0).astype(bf16)
            scores = scores + dot_nt(only, r.kvbuf[4 * g + i])
            length = jnp.where(row_pair == i, r.lengths[4 * g + i], length)
        gates = jnp.concatenate([r.gates[4 * g + i] for i in range(4)], axis=0)
        last_gate = jnp.sum(
            jnp.where(position == length - 1, gates, 0.0), axis=-1, keepdims=True
        )
        bias = last_gate - gates + gate_new[at]
        cached = jnp.where(position < length, jnp.exp(scores * scale + bias), 0.0)
        whole = jnp.sum(cached, axis=-1, keepdims=True) + own_exp[at]
        probs = (cached / whole).astype(bf16)
        got = (own_exp[at] / whole).astype(bf16).astype(f32) * kv_pairs[at]
        for i in range(4):
            got = got + jnp.where(row_pair_wide == i, dot(probs, r.kvbuf[4 * g + i]), 0.0)
        r.att[at] = got
    attended = jnp.where(
        low_lanes,
        pltpu.roll(r.att[pl.ds(0, seq, stride=2)], hd, 1),
        r.att[pl.ds(1, seq, stride=2)],
    ).astype(bf16)
    late[1].wait()

    r.part[ny - 1] = dot(attended, r.wo[...]).astype(bf16)
    for d in y_order:
        go("s_part", r.part.at[ny - 1], r.part.at[d - 1], r.s1r, tp=yp(d))
    arrived(r.part.at[pl.ds(0, ny - 1)], r.s1r)
    total = jnp.zeros((seq, d_model), f32)
    for j in range(ny):
        total = total + r.part[yp(-j - 1)].astype(f32)
    res = r.tok[...].astype(f32) + total.astype(bf16).astype(f32)
    for j in range(ny):
        r.resid[j] = res[j * rows4 : (j + 1) * rows4]
    mine = h_all.at[blk(c, z, x)]
    hidden = rms_scaled(res, r.gain2[...]).astype(bf16)
    common = d_model // 2
    lanes_tp = fq // 2
    wide_at = common + META
    mine[:, :common] = hidden[:, :common]
    mine[:, common:wide_at] = meta.astype(bf16)
    for j in range(ny):
        r.hid[j] = hidden[:, common + j * lanes_tp : common + (j + 1) * lanes_tp]
    mine[:, wide_at:] = r.hid[t]

    for d in range(1, NX):
        go("s_x", mine, mine, r.xrs.at[d - 1], ep=ep_at(z, xp(d), c))

    half = (NX + 1) // 2
    last = NZ // 2

    def takes(direction, step, q):
        if step < last:
            return True
        return q < half if direction > 0 else q >= half

    def pass_on(direction, step, q):
        if step > last or not takes(direction, step, q):
            return
        block = h_all.at[blk(c, zp(-direction * (step - 1)), xp(-q))]
        rs = r.rrs if direction > 0 else r.lrs
        go("s_ring", block, block, rs.at[step - 1, q], ep=ep_at(zp(direction), x, c))

    def across(rel, q):
        block = h_all.at[blk(c, zp(rel), xp(-q))]
        go("s_core", block, block, r.dcr.at[rel % NZ], ep=ep_at(z, x, cp(1)))

    others = pl.ds(1, ny - 1)

    def row_at(ci, rel):
        return pl.ds(blk(ci, zp(rel), 0), NX)

    def give_tp(rel):
        here = h_all.at[row_at(c, rel), :, pl.ds(wide_at, lanes_tp)]
        for d in y_order:
            go("s_tp", here, r.h_tp.at[d, row_at(c, rel)], r.tpr.at[rel % NZ], tp=yp(d))

    def take_tp(rel):
        there = r.h_tp.at[others, row_at(c, rel)]
        arrived(there, r.tpr.at[rel % NZ])
        go("s_tpcore", there, there, r.dtr.at[rel % NZ], ep=ep_at(z, x, cp(1)))

    def from_other_core(rel):
        arrived(h_all.at[row_at(cp(1), rel)], r.dcr.at[rel % NZ])
        arrived(r.h_tp.at[others, row_at(cp(1), rel)], r.dtr.at[rel % NZ])
        for ci in range(NC):
            at = pl.ds(blk(ci, zp(rel), 0), NX)
            r.h_tp[0, at] = h_all[at, :, wide_at:]

    def z_step(step):
        for q in range(NX):
            for direction in (1, -1):
                if not takes(direction, step, q):
                    continue
                rs = r.rrs if direction > 0 else r.lrs
                arrived(h_all.at[blk(c, zp(-direction * step), xp(-q))], rs.at[step - 1, q])
                pass_on(direction, step + 1, q)
                across(-direction * step, q)

    def features_of(zi):
        rows = []
        for ci in range(NC):
            at = pl.ds(blk(ci, zi, 0), NX)
            parts = [h_all[at, :, :common]] + [r.h_tp[yp(-j), at] for j in range(ny)]
            rows.append(jnp.concatenate(parts, axis=-1).reshape(per_z, d_model))
        return jnp.concatenate(rows, axis=0)

    def codes_of(zi):
        parts = [h_all[pl.ds(blk(ci, zi, 0), NX), :, common:wide_at] for ci in range(NC)]
        return jnp.concatenate([v.reshape(per_z, META) for v in parts], axis=0)

    in_first = iota((per_z, 2 * units), 1) < units

    def dense_units(rel):
        zi = zp(rel)
        pre = dot_nt(features_of(zi), r.wgu[...])
        low, high = pre[:per_z], pre[per_z:]
        act = clamped_unit(
            jnp.where(in_first, low, pltpu.roll(high, units, 1)),
            jnp.where(in_first, pltpu.roll(low, units, 1), high),
        ).astype(bf16)
        d = rel % NZ
        if d == 0:
            r.arecv[NZ - 1] = act
            return
        r.asend[d - 1] = act
        go("s_act", r.asend.at[d - 1], r.arecv.at[d - 1], r.ars, ep=ep_at(zi, x, c))

    lead8 = jnp.where(iota((8, META), 0) == iota((8, META), 1), 1.0, 0.0).astype(bf16)
    code_base = (ep * 4).astype(f32)

    def pick_rows(rel):
        zi = zp(rel)
        codes = dot_nt(lead8, codes_of(zi))
        block = iota((1, both_z), 1) // seq
        where = ((block % NX) * NC + block // NX).astype(f32)
        target = jnp.full((1, both_z), -1.0, f32)
        for k in range(top):
            j = codes[k : k + 1] - code_base
            target = jnp.where((j >= 0.0) & (j <= CAP - 1.0), where + j * nxc, target)
        slot = iota((zrows, both_z), 0).astype(f32)
        return dot(jnp.where(slot == target, 1.0, 0.0).astype(bf16), features_of(zi))

    def experts_of(rels, send=True):
        start = min(i for i, rel in enumerate(z_order) if rel in rels) * zrows
        rows = len(rels) * zrows
        for i, rel in enumerate(rels):
            r.xs[start + i * zrows : start + (i + 1) * zrows] = pick_rows(rel)
        xs = r.xs[start : start + rows].astype(bf16)
        act = clamped_unit(dot(xs, r.eg[...]), dot(xs, r.eu[...])).astype(bf16)
        for d in y_order + [0]:
            peer = yp(d)
            made = dot(act, r.ed[:, pl.ds(pl.multiple_of(peer * fq, fq), fq)])
            for i, rel in enumerate(rels):
                piece = made[i * zrows : (i + 1) * zrows]
                if d == 0:
                    r.rown[rel % NZ] = piece
                    continue
                r.ysend[d - 1, rel % NZ] = piece.astype(bf16)
            if d and send:
                send_results(rels, d)

    def send_results(rels, d):
        for rel in rels:
            i = rel % NZ
            go("s_y", r.ysend.at[d - 1, i], r.yrecv.at[i, d - 1], r.yrs.at[i], tp=yp(d))

    def finish(rels):
        for rel in rels:
            d = rel % NZ
            arrived(r.yrecv.at[d], r.yrs.at[d])
            summed = r.rown[d]
            for i in range(ny - 1):
                summed = summed + r.yrecv[d, i].astype(f32)
            if d == 0:
                r.zr[NZ - 1] = summed.astype(bf16)
                continue
            r.zs[d - 1] = summed.astype(bf16)
            go("s_z", r.zs.at[d - 1], r.zr.at[d - 1], r.zrs, ep=ep_at(zp(d), x, c))

    z_order = [0]
    for step in range(1, last):
        z_order += [-step, step]
    z_order.append(last)

    for q in range(NX):
        if q:
            arrived(h_all.at[blk(c, z, xp(-q))], r.xrs.at[q - 1])
        pass_on(1, 1, q)
        pass_on(-1, 1, q)
        across(0, q)
    give_tp(0)
    for load in late[2:]:
        load.wait()
    z_step(1)
    give_tp(-1)
    if last > 1:
        give_tp(1)
    take_tp(0)

    parts = [[0, -1, 1], [-2, 2], [-3, 3, 4]] if NZ == 8 else [z_order]
    for step in range(2, last + 1):
        z_step(step)
        give_tp(-step)
        if step < last:
            give_tp(step)
        take_tp(1 - step)
        take_tp(step - 1)
        if NZ != 8:
            continue
        if step == 4:
            for d in y_order:
                send_results(parts[0], d)
        if step == 2:
            from_other_core(0)
            dense_units(0)
        elif step == 3:
            from_other_core(-1)
            from_other_core(1)
            dense_units(-1)
            dense_units(1)
            experts_of(parts[0], send=False)
        else:
            from_other_core(-2)
            from_other_core(2)
            experts_of(parts[1])
            dense_units(-2)
            dense_units(2)
    own_meta = codes_of(z).astype(f32)
    mix = jnp.sum(features_of(z).astype(f32) * r.dmix[...], axis=-1, keepdims=True)
    mix = jax.nn.sigmoid(mix)
    col = iota((1, slots), 1)
    col_block = col // nxc
    col_z = (col_block * 43) // 128
    targets = 4 * (col_z * nxc + x * NC + c) + (col_block - CAP * col_z)
    targets = targets.astype(f32)
    row_block = iota((both_z, 1), 0) // seq
    row_xc = (row_block % NX) * NC + row_block // NX
    spread = jnp.zeros((both_z, slots), f32)
    for k in range(top):
        weight = (
            own_meta[:, top + k : top + k + 1]
            + own_meta[:, 2 * top + k : 2 * top + k + 1]
            + own_meta[:, 3 * top + k : 3 * top + k + 1]
        )
        spread = spread + jnp.where(own_meta[:, k : k + 1] == targets, weight, 0.0)
    spread = jnp.where(row_xc == col % nxc, spread, 0.0)
    spread_high = spread.astype(bf16)
    spread_low = (spread - spread_high.astype(f32)).astype(bf16)

    take_tp(last)
    for rel in parts[-1]:
        from_other_core(rel)
    experts_of(parts[-1])
    for part in parts[:-1]:
        finish(part)
    for rel in reversed(z_order[5:] if NZ == 8 else z_order):
        dense_units(rel)

    finish(parts[-1])

    arrived(r.dd.at[pl.ds(0, NZ - 1)], r.ddr)
    arrived(r.arecv.at[pl.ds(0, NZ - 1)], r.ars)
    dense = jnp.zeros((both_z, fq), f32)
    for j in range(NZ):
        got = r.arecv[j].astype(f32)
        both = jnp.concatenate(
            [jnp.where(in_first, got, 0.0), jnp.where(in_first, 0.0, got)], axis=0
        ).astype(bf16)
        twice = jnp.concatenate([r.dd[j], r.dd[j]], axis=0)
        dense = dense + dot(both, twice)
    dense = mix * dense
    arrived(r.zr.at[pl.ds(0, NZ - 1)], r.zrs)
    for j in range(NZ):
        r.zf[j * zrows : (j + 1) * zrows] = r.zr[lax.rem(z - j - 1 + 2 * NZ, NZ)].astype(f32)
    results = r.zf[...].astype(bf16)
    mixed = dot(spread_high, results) + dot(spread_low, results) + dense
    for i in range(nxc * ny):
        r.cs[i] = mixed[i * rows4 : (i + 1) * rows4].astype(bf16)

    for i, (dt, dx, dc) in enumerate(plane):
        here = (cp(dc) * NX + xp(dx)) * ny + yp(dt)
        go(
            "s_out",
            r.cs.at[here],
            r.cr.at[i + 1],
            r.crs,
            ep=ep_at(z, xp(dx), cp(dc)),
            tp=yp(dt),
        )
    r.cr[0] = r.cs[(c * NX + x) * ny + t]
    res = r.resid[t]
    arrived(r.cr.at[pl.ds(1, len(plane))], r.crs)
    for j in range(ny):
        cols = slice(j * fq, (j + 1) * fq)
        moved = r.cr[pl.ds(yp(-j) * nxc, nxc)].astype(f32)
        r.out[:, cols] = (res[:, cols] + jnp.sum(moved, axis=0)).astype(bf16)
    sizes = dict(
        s_dd=r.dd,
        s_part=r.part,
        s_x=h_all,
        s_ring=h_all,
        s_core=h_all,
        s_tpcore=None,
        s_tp=None,
        s_act=r.asend,
        s_z=r.zs,
        s_out=r.cr,
    )
    for key, count in sent.items():
        if key == "s_y":
            whole = r.ysend
        elif key == "s_tp":
            whole = r.h_tp.at[others, pl.ds(0, NX * NZ)]
        elif key == "s_tpcore":
            whole = r.h_tp.at[others, pl.ds(0, NX * count)]
        else:
            whole = sizes[key].at[pl.ds(0, count)]
        remote(whole, whole, getattr(r, key), r.crs, ep=ep, tp=t).wait_send()


def on_device(
    tokens,
    norm1_gain,
    query_weight,
    key_weight,
    value_weight,
    forget_weight,
    forget_bias,
    out_weight,
    kv_cache,
    log_gates,
    lengths,
    norm2_gain,
    routing,
    route_weight,
    expert_gate,
    expert_up,
    expert_down,
    dense_gate,
    dense_up,
    dense_down,
    dense_mix,
):
    seq, d_model = tokens.shape
    top = routing.shape[1]
    ny = lax.axis_size("tp")
    rows4 = seq // ny
    ff = expert_gate.shape[2]
    units = dense_gate.shape[1]
    fq = d_model // ny
    nxc = NX * NC
    nblk = NC * NZ * NX
    zrows = CAP * nxc
    slots = NZ * zrows
    width = d_model // 2 + META + fq // 2
    last = NZ // 2
    f32, bf16 = jnp.float32, jnp.bfloat16
    hd2 = kv_cache.shape[3]
    vm = pltpu.VMEM

    def dma(*shape):
        return pltpu.SemaphoreType.DMA(shape) if shape else pltpu.SemaphoreType.DMA

    scratch = dict(
        h_all=vm((nblk, seq, width), bf16),
        h_tp=vm((ny, nblk, seq, fq // 2), bf16),
        hid=vm((ny, seq, fq // 2), bf16),
        kvbuf=vm((seq, kv_cache.shape[1], hd2), bf16),
        wkv=vm((hd2, d_model), bf16),
        wo=vm((hd2, d_model), bf16),
        att=vm((2 * seq, hd2), f32),
        part=vm((ny, seq, d_model), bf16),
        resid=vm((ny, rows4, d_model), f32),
        eg=vm((d_model, ff), bf16),
        eu=vm((d_model, ff), bf16),
        ed=vm((ff, d_model), bf16),
        wgu=vm((2 * units, d_model), bf16),
        dd=vm((NZ, units, fq), bf16),
        xs=vm((slots, d_model), f32),
        ysend=vm((ny - 1, NZ, zrows, fq), bf16),
        yrecv=vm((NZ, ny - 1, zrows, fq), bf16),
        rown=vm((NZ, zrows, fq), f32),
        zs=vm((NZ - 1, zrows, fq), bf16),
        zr=vm((NZ, zrows, fq), bf16),
        zf=vm((slots, fq), f32),
        asend=vm((NZ - 1, NX * seq, 2 * units), bf16),
        arecv=vm((NZ, NX * seq, 2 * units), bf16),
        cs=vm((nxc * ny, rows4, fq), bf16),
        cr=vm((nxc * ny, rows4, fq), bf16),
        kvsem=dma(4),
        ldsem=dma(7),
        s1r=dma(),
        xrs=dma(max(NX - 1, 1)),
        rrs=dma(last, NX),
        lrs=dma(last, NX),
        dcr=dma(NZ),
        tpr=dma(NZ),
        dtr=dma(NZ),
        ddr=dma(),
        yrs=dma(NZ),
        zrs=dma(),
        ars=dma(),
        crs=dma(),
        s_dd=dma(),
        s_part=dma(),
        s_x=dma(),
        s_ring=dma(),
        s_core=dma(),
        s_tp=dma(),
        s_tpcore=dma(),
        s_act=dma(),
        s_y=dma(),
        s_z=dma(),
        s_out=dma(),
    )
    in_vmem = pl.BlockSpec(memory_space=pltpu.VMEM)
    in_smem = pl.BlockSpec(memory_space=pltpu.SMEM)
    in_hbm = pl.BlockSpec(memory_space=pl.ANY)
    places = [in_vmem] * VMEM_INPUTS + [in_hbm] * (len(IN_NAMES) - VMEM_INPUTS)
    places[IN_NAMES.index("lengths")] = in_smem
    places[IN_NAMES.index("fbias")] = in_smem
    names = tuple(IN_NAMES) + ("out",) + tuple(scratch)
    return pl.pallas_call(
        functools.partial(layer_kernel, names, top),
        out_shape=jax.ShapeDtypeStruct((rows4, d_model), bf16),
        in_specs=places,
        out_specs=in_vmem,
        scratch_shapes=list(scratch.values()),
        compiler_params=pltpu.CompilerParams(
            collective_id=0, has_side_effects=True, vmem_limit_bytes=60 * 1024 * 1024
        ),
        name="layer",
    )(
        tokens,
        norm1_gain.reshape(1, d_model),
        norm2_gain.reshape(1, d_model),
        dense_mix.reshape(1, d_model),
        query_weight,
        key_weight.T,
        value_weight.T,
        forget_weight.T,
        forget_bias.reshape(1, -1),
        lengths,
        log_gates,
        routing.T,
        route_weight.T,
        out_weight,
        kv_cache.reshape(seq, kv_cache.shape[1], hd2),
        expert_gate[0],
        expert_up[0],
        expert_down[0],
        dense_gate.T,
        dense_up.T,
        dense_down,
    )


def solution(mesh):
    return jax.shard_map(
        on_device,
        mesh=mesh,
        in_specs=(
            P("ep", None),
            P(),
            P(None, "tp"),
            P(None, "tp"),
            P(None, "tp"),
            P(None, "tp"),
            P("tp"),
            P("tp", None),
            P("ep", None, "tp", None),
            P("ep", "tp", None),
            P("ep"),
            P(),
            P("ep", None),
            P("ep", None),
            P("ep", None, "tp"),
            P("ep", None, "tp"),
            P("ep", "tp", None),
            P(None, "ep"),
            P(None, "ep"),
            P("ep", None),
            P(),
        ),
        out_specs=P(("ep", "tp"), None),
        check_vma=False,
    )
```

```python
import functools

import jax
import jax.numpy as jnp
from jax import lax
from jax.experimental import pallas as pl
from jax.experimental.pallas import tpu as pltpu
from jax.sharding import PartitionSpec as P

EPS = 1e-05
LIMIT = 7.0
ALPHA = 1.702
NZ, NX, NC = 8, 4, 2
CAP = 3
META = 128
MESH = pl.DeviceIdType.MESH


def clamped_unit(gate_pre, up_pre):
    capped = jnp.minimum(gate_pre, LIMIT)
    return capped * jax.nn.sigmoid(ALPHA * capped) * (jnp.clip(up_pre, -LIMIT, LIMIT) + 1.0)


def rms_scaled(values, gain_vec):
    return values * lax.rsqrt(jnp.mean(values * values, axis=-1, keepdims=True) + EPS) * gain_vec


def remote(src, dst, send_sem, recv_sem, **device):
    return pltpu.make_async_remote_copy(
        src_ref=src,
        dst_ref=dst,
        send_sem=send_sem,
        recv_sem=recv_sem,
        device_id=device,
        device_id_type=MESH,
    )


IN_NAMES = (
    "tok",
    "gain1",
    "gain2",
    "dmix",
    "fwt",
    "fbias",
    "lengths",
    "gates",
    "routing",
    "weight",
    "wout",
    "kv",
    "wq_hbm",
    "wkt",
    "wvt",
    "eg_hbm",
    "eu_hbm",
    "ed_hbm",
    "dgt",
    "dut",
    "dd_hbm",
)
VMEM_INPUTS = 10


class Refs:
    pass


def layer_kernel(names, top, *refs):
    r = Refs()
    for name, ref in zip(names, refs, strict=True):
        setattr(r, name, ref)
    seq, d_model = r.tok.shape
    ny = r.part.shape[0]
    rows4 = seq // ny
    nblk = NC * NZ * NX
    fq = d_model // ny
    nxc = NX * NC
    zrows = CAP * nxc
    slots = NZ * zrows
    per_z = NX * seq
    both_z = NC * per_z
    f32, bf16 = jnp.float32, jnp.bfloat16
    h_all = r.h_all
    ep = lax.axis_index("ep")
    t = lax.axis_index("tp")
    z = ep // nxc
    x = (ep // NC) % NX
    c = ep % NC

    def ep_at(zi, xi, ci):
        return (zi * NX + xi) * NC + ci

    def blk(ci, zi, xi):
        return (ci * NZ + zi) * NX + xi

    def yp(d):
        return lax.rem(t + d + ny, ny)

    def zp(d):
        return lax.rem(z + d + NZ, NZ)

    def xp(d):
        return lax.rem(x + d + NX, NX)

    def cp(d):
        return lax.rem(c + d, NC)

    def iota(shape, dim):
        return lax.broadcasted_iota(jnp.int32, shape, dim)

    def dot_nt(a, b):
        return lax.dot_general(a, b, (((1,), (1,)), ((), ())), preferred_element_type=f32)

    def dot(a, b):
        return jnp.dot(a, b, preferred_element_type=f32)

    y_order = sorted(range(1, ny), key=lambda d: -min(d, ny - d))

    hd = r.wkt.shape[0]
    early = [
        pltpu.make_async_copy(r.wq_hbm, r.wq, r.qsem.at[0]),
        pltpu.make_async_copy(r.wkt, r.wkv.at[pl.ds(0, hd)], r.qsem.at[1]),
        pltpu.make_async_copy(r.wvt, r.wkv.at[pl.ds(hd, hd)], r.qsem.at[2]),
    ]
    for load in early:
        load.start()
    barrier = pltpu.get_barrier_semaphore()
    plane = [(dt, dx, dc) for dt in range(ny) for dc in range(NC) for dx in range(NX)][1:]
    for dt, dx, dc in plane:
        pl.semaphore_signal(
            barrier,
            inc=1,
            device_id={"ep": ep_at(z, xp(dx), cp(dc)), "tp": yp(dt)},
            device_id_type=MESH,
        )
    for d in range(1, NZ):
        pl.semaphore_signal(
            barrier, inc=1, device_id={"ep": ep_at(zp(d), x, c)}, device_id_type=MESH
        )

    units = r.dgt.shape[0]
    kv_groups = 4
    per_group = seq // kv_groups
    kv_loads = [
        pltpu.make_async_copy(
            r.kv.at[pl.ds(i * per_group, per_group)],
            r.kvbuf.at[pl.ds(i * per_group, per_group)],
            r.kvsem.at[i],
        )
        for i in range(kv_groups)
    ]
    late = [
        (r.dd_hbm.at[:, pl.ds(pl.multiple_of(t * fq, fq), fq)], r.dd.at[NZ - 1]),
        (r.wout, r.wo),
        (r.dgt, r.wgu.at[pl.ds(0, units)]),
        (r.dut, r.wgu.at[pl.ds(units, units)]),
        (r.eg_hbm, r.eg),
        (r.eu_hbm, r.eu),
        (r.ed_hbm, r.ed),
    ]
    late = [pltpu.make_async_copy(src, dst, r.ldsem.at[i]) for i, (src, dst) in enumerate(late)]
    for load in kv_loads + late:
        load.start()

    sent = {}

    def go(key, src, dst, recv_sem, **device):
        remote(src, dst, getattr(r, key), recv_sem, **device).start()
        sent[key] = sent.get(key, 0) + 1

    def arrived(ref, recv_sem):
        remote(ref, ref, r.s_dd, recv_sem, ep=ep, tp=t).wait_recv()

    tok = r.tok[...].astype(f32)
    normed = rms_scaled(tok, r.gain1[...])
    normed = normed.astype(bf16)
    for load in early:
        load.wait()
    cache_len = r.kv.shape[1]
    scale = hd ** (-0.5)
    q = dot(normed, r.wq[...]).astype(bf16).astype(f32)
    kv_new = dot_nt(normed, r.wkv[...]).astype(bf16).astype(f32)
    low_lanes = iota((seq, 2 * hd), 1) < hd
    q_heads = [jnp.where(low_lanes, q, 0.0), jnp.where(low_lanes, pltpu.roll(q, hd, 1), 0.0)]
    wide = normed.astype(f32)
    pairs = 2 * seq
    of_pair = iota((pairs, seq), 0) == 2 * iota((pairs, seq), 1)
    of_pair1 = iota((pairs, seq), 0) == 2 * iota((pairs, seq), 1) + 1
    eye = jnp.where(iota((seq, seq), 0) == iota((seq, seq), 1), 1.0, 0.0)

    def to_pairs(first, second):
        rows = [jnp.sum(eye * v, axis=0, keepdims=True) for v in (first, second)]
        return jnp.sum(
            jnp.where(of_pair, rows[0], jnp.where(of_pair1, rows[1], 0.0)), axis=1, keepdims=True
        )

    of_heads = [jnp.where(m, 1.0, 0.0).astype(bf16) for m in (of_pair, of_pair1)]
    q_pairs = sum(dot(of_heads[h], q_heads[h].astype(bf16)) for h in range(2))
    kv_pairs = dot(of_heads[0] + of_heads[1], kv_new.astype(bf16))
    gate_new, own_exp = [], []
    for h in range(2):
        pre = jnp.sum(wide * r.fwt[h : h + 1, :].astype(f32), axis=-1, keepdims=True)
        pre = pre + r.fbias[0, h]
        gate_new.append(jnp.minimum(pre, 0.0) - jnp.log(1.0 + jnp.exp(-jnp.abs(pre))))
        own_exp.append(jnp.exp(jnp.sum(q_heads[h] * kv_new, axis=-1, keepdims=True) * scale))
    gate_new = to_pairs(*gate_new)
    own_exp = to_pairs(*own_exp)

    rt = r.routing[...].astype(f32)
    wt = r.weight[...]
    earlier = iota((seq, seq), 1) < iota((seq, seq), 0)
    lane = iota((seq, META), 1)
    meta = jnp.zeros((seq, META), f32)

    def column(row):
        return jnp.sum(eye * row, axis=-1, keepdims=True)

    for k in range(top):
        chosen = column(rt[k : k + 1])
        same = jnp.zeros((seq, seq), f32)
        for other in range(top):
            same = same + jnp.where((chosen == rt[other : other + 1]) & earlier, 1.0, 0.0)
        rank = jnp.sum(same, axis=-1, keepdims=True)
        value = column(wt[k : k + 1])
        high = value.astype(bf16).astype(f32)
        mid = (value - high).astype(bf16).astype(f32)
        parts = (4.0 * chosen + rank, high, mid, value - high - mid)
        for i, v in enumerate(parts):
            meta = jnp.where(lane == i * top + k, v, meta)

    position = iota((8, cache_len), 1)
    row_pair = iota((8, 1), 0) // 2
    row_pair_wide = iota((8, 2 * hd), 0) // 2

    for g in range(kv_groups):
        kv_loads[g].wait()
        if g == 0:
            pl.semaphore_wait(barrier, len(plane) + (NZ - 1))
            late[0].wait()
            for d in range(1, NZ):
                go("s_dd", r.dd.at[NZ - 1], r.dd.at[d - 1], r.ddr, ep=ep_at(zp(d), x, c))
        at = slice(8 * g, 8 * g + 8)
        queries = q_pairs[at]
        scores = jnp.zeros((8, cache_len), f32)
        length = jnp.zeros((8, 1), jnp.int32)
        for i in range(4):
            only = jnp.where(row_pair_wide == i, queries, 0.0).astype(bf16)
            scores = scores + dot_nt(only, r.kvbuf[4 * g + i])
            length = jnp.where(row_pair == i, r.lengths[4 * g + i], length)
        gates = jnp.concatenate([r.gates[4 * g + i] for i in range(4)], axis=0)
        last_gate = jnp.sum(
            jnp.where(position == length - 1, gates, 0.0), axis=-1, keepdims=True
        )
        bias = last_gate - gates + gate_new[at]
        cached = jnp.where(position < length, jnp.exp(scores * scale + bias), 0.0)
        whole = jnp.sum(cached, axis=-1, keepdims=True) + own_exp[at]
        probs = (cached / whole).astype(bf16)
        got = (own_exp[at] / whole).astype(bf16).astype(f32) * kv_pairs[at]
        for i in range(4):
            got = got + jnp.where(row_pair_wide == i, dot(probs, r.kvbuf[4 * g + i]), 0.0)
        r.att[at] = got
    attended = jnp.where(
        low_lanes,
        pltpu.roll(r.att[pl.ds(0, seq, stride=2)], hd, 1),
        r.att[pl.ds(1, seq, stride=2)],
    ).astype(bf16)
    late[1].wait()

    r.part[ny - 1] = dot(attended, r.wo[...]).astype(bf16)
    for d in y_order:
        go("s_part", r.part.at[ny - 1], r.part.at[d - 1], r.s1r, tp=yp(d))
    arrived(r.part.at[pl.ds(0, ny - 1)], r.s1r)
    total = jnp.zeros((seq, d_model), f32)
    for j in range(ny):
        total = total + r.part[yp(-j - 1)].astype(f32)
    res = r.tok[...].astype(f32) + total.astype(bf16).astype(f32)
    for j in range(ny):
        r.resid[j] = res[j * rows4 : (j + 1) * rows4]
    mine = h_all.at[blk(c, z, x)]
    hidden = rms_scaled(res, r.gain2[...]).astype(bf16)
    common = d_model // 2
    lanes_tp = fq // 2
    wide_at = common + META
    mine[:, :common] = hidden[:, :common]
    mine[:, common:wide_at] = meta.astype(bf16)
    for j in range(ny):
        r.hid[j] = hidden[:, common + j * lanes_tp : common + (j + 1) * lanes_tp]
    mine[:, wide_at:] = r.hid[t]

    for d in range(1, NX):
        go("s_x", mine, mine, r.xrs.at[d - 1], ep=ep_at(z, xp(d), c))

    half = (NX + 1) // 2
    last = NZ // 2

    def takes(direction, step, q):
        if step < last:
            return True
        return q < half if direction > 0 else q >= half

    def pass_on(direction, step, q):
        if step > last or not takes(direction, step, q):
            return
        block = h_all.at[blk(c, zp(-direction * (step - 1)), xp(-q))]
        rs = r.rrs if direction > 0 else r.lrs
        go("s_ring", block, block, rs.at[step - 1, q], ep=ep_at(zp(direction), x, c))

    def across(rel, q):
        block = h_all.at[blk(c, zp(rel), xp(-q))]
        go("s_core", block, block, r.dcr.at[rel % NZ], ep=ep_at(z, x, cp(1)))

    others = pl.ds(1, ny - 1)

    def row_at(ci, rel):
        return pl.ds(blk(ci, zp(rel), 0), NX)

    def give_tp(rel):
        here = h_all.at[row_at(c, rel), :, pl.ds(wide_at, lanes_tp)]
        for d in y_order:
            go("s_tp", here, r.h_tp.at[d, row_at(c, rel)], r.tpr.at[rel % NZ], tp=yp(d))

    def take_tp(rel):
        there = r.h_tp.at[others, row_at(c, rel)]
        arrived(there, r.tpr.at[rel % NZ])
        go("s_tpcore", there, there, r.dtr.at[rel % NZ], ep=ep_at(z, x, cp(1)))

    def from_other_core(rel):
        arrived(h_all.at[row_at(cp(1), rel)], r.dcr.at[rel % NZ])
        arrived(r.h_tp.at[others, row_at(cp(1), rel)], r.dtr.at[rel % NZ])
        for ci in range(NC):
            at = pl.ds(blk(ci, zp(rel), 0), NX)
            r.h_tp[0, at] = h_all[at, :, wide_at:]

    def z_step(step):
        for q in range(NX):
            for direction in (1, -1):
                if not takes(direction, step, q):
                    continue
                rs = r.rrs if direction > 0 else r.lrs
                arrived(h_all.at[blk(c, zp(-direction * step), xp(-q))], rs.at[step - 1, q])
                pass_on(direction, step + 1, q)
                across(-direction * step, q)

    def features_of(zi):
        rows = []
        for ci in range(NC):
            at = pl.ds(blk(ci, zi, 0), NX)
            parts = [h_all[at, :, :common]] + [r.h_tp[yp(-j), at] for j in range(ny)]
            rows.append(jnp.concatenate(parts, axis=-1).reshape(per_z, d_model))
        return jnp.concatenate(rows, axis=0)

    def codes_of(zi):
        parts = [h_all[pl.ds(blk(ci, zi, 0), NX), :, common:wide_at] for ci in range(NC)]
        return jnp.concatenate([v.reshape(per_z, META) for v in parts], axis=0)

    in_first = iota((per_z, 2 * units), 1) < units

    def dense_units(rel):
        zi = zp(rel)
        pre = dot_nt(features_of(zi), r.wgu[...])
        low, high = pre[:per_z], pre[per_z:]
        act = clamped_unit(
            jnp.where(in_first, low, pltpu.roll(high, units, 1)),
            jnp.where(in_first, pltpu.roll(low, units, 1), high),
        ).astype(bf16)
        d = rel % NZ
        if d == 0:
            r.arecv[NZ - 1] = act
            return
        r.asend[d - 1] = act
        go("s_act", r.asend.at[d - 1], r.arecv.at[d - 1], r.ars, ep=ep_at(zi, x, c))

    lead8 = jnp.where(iota((8, META), 0) == iota((8, META), 1), 1.0, 0.0).astype(bf16)
    code_base = (ep * 4).astype(f32)

    def pick_rows(rel):
        zi = zp(rel)
        codes = dot_nt(lead8, codes_of(zi))
        block = iota((1, both_z), 1) // seq
        where = ((block % NX) * NC + block // NX).astype(f32)
        target = jnp.full((1, both_z), -1.0, f32)
        for k in range(top):
            j = codes[k : k + 1] - code_base
            target = jnp.where((j >= 0.0) & (j <= CAP - 1.0), where + j * nxc, target)
        slot = iota((zrows, both_z), 0).astype(f32)
        return dot(jnp.where(slot == target, 1.0, 0.0).astype(bf16), features_of(zi))

    def experts_of(rels, send=True):
        start = min(i for i, rel in enumerate(z_order) if rel in rels) * zrows
        rows = len(rels) * zrows
        for i, rel in enumerate(rels):
            r.xs[start + i * zrows : start + (i + 1) * zrows] = pick_rows(rel)
        xs = r.xs[start : start + rows].astype(bf16)
        act = clamped_unit(dot(xs, r.eg[...]), dot(xs, r.eu[...])).astype(bf16)
        for d in y_order + [0]:
            peer = yp(d)
            made = dot(act, r.ed[:, pl.ds(pl.multiple_of(peer * fq, fq), fq)])
            for i, rel in enumerate(rels):
                piece = made[i * zrows : (i + 1) * zrows]
                if d == 0:
                    r.rown[rel % NZ] = piece
                    continue
                r.ysend[d - 1, rel % NZ] = piece.astype(bf16)
            if d and send:
                send_results(rels, d)

    def send_results(rels, d):
        for rel in rels:
            i = rel % NZ
            go("s_y", r.ysend.at[d - 1, i], r.yrecv.at[i, d - 1], r.yrs.at[i], tp=yp(d))

    def finish(rels):
        for rel in rels:
            d = rel % NZ
            arrived(r.yrecv.at[d], r.yrs.at[d])
            summed = r.rown[d]
            for i in range(ny - 1):
                summed = summed + r.yrecv[d, i].astype(f32)
            if d == 0:
                r.zr[NZ - 1] = summed.astype(bf16)
                continue
            r.zs[d - 1] = summed.astype(bf16)
            go("s_z", r.zs.at[d - 1], r.zr.at[d - 1], r.zrs, ep=ep_at(zp(d), x, c))

    z_order = [0]
    for step in range(1, last):
        z_order += [-step, step]
    z_order.append(last)

    for q in range(NX):
        if q:
            arrived(h_all.at[blk(c, z, xp(-q))], r.xrs.at[q - 1])
        pass_on(1, 1, q)
        pass_on(-1, 1, q)
        across(0, q)
    give_tp(0)
    for load in late[2:]:
        load.wait()
    z_step(1)
    give_tp(-1)
    if last > 1:
        give_tp(1)
    take_tp(0)

    parts = [[0, -1, 1], [-2, 2], [-3, 3, 4]] if NZ == 8 else [z_order]
    for step in range(2, last + 1):
        z_step(step)
        give_tp(-step)
        if step < last:
            give_tp(step)
        take_tp(1 - step)
        take_tp(step - 1)
        if NZ != 8:
            continue
        if step == 4:
            for d in y_order:
                send_results(parts[0], d)
        if step == 2:
            from_other_core(0)
            dense_units(0)
        elif step == 3:
            from_other_core(-1)
            from_other_core(1)
            dense_units(-1)
            dense_units(1)
            experts_of(parts[0], send=False)
        else:
            from_other_core(-2)
            from_other_core(2)
            experts_of(parts[1])
            dense_units(-2)
            dense_units(2)
    own_meta = codes_of(z).astype(f32)
    mix = jnp.sum(features_of(z).astype(f32) * r.dmix[...], axis=-1, keepdims=True)
    mix = jax.nn.sigmoid(mix)
    col = iota((1, slots), 1)
    col_block = col // nxc
    col_z = (col_block * 43) // 128
    targets = 4 * (col_z * nxc + x * NC + c) + (col_block - CAP * col_z)
    targets = targets.astype(f32)
    row_block = iota((both_z, 1), 0) // seq
    row_xc = (row_block % NX) * NC + row_block // NX
    spread = jnp.zeros((both_z, slots), f32)
    for k in range(top):
        weight = (
            own_meta[:, top + k : top + k + 1]
            + own_meta[:, 2 * top + k : 2 * top + k + 1]
            + own_meta[:, 3 * top + k : 3 * top + k + 1]
        )
        spread = spread + jnp.where(own_meta[:, k : k + 1] == targets, weight, 0.0)
    spread = jnp.where(row_xc == col % nxc, spread, 0.0)
    spread_high = spread.astype(bf16)
    spread_low = (spread - spread_high.astype(f32)).astype(bf16)

    take_tp(last)
    for rel in parts[-1]:
        from_other_core(rel)
    experts_of(parts[-1])
    for part in parts[:-1]:
        finish(part)
    for rel in reversed(z_order[5:] if NZ == 8 else z_order):
        dense_units(rel)

    finish(parts[-1])

    arrived(r.dd.at[pl.ds(0, NZ - 1)], r.ddr)
    arrived(r.arecv.at[pl.ds(0, NZ - 1)], r.ars)
    dense = jnp.zeros((both_z, fq), f32)
    for j in range(NZ):
        got = r.arecv[j].astype(f32)
        both = jnp.concatenate(
            [jnp.where(in_first, got, 0.0), jnp.where(in_first, 0.0, got)], axis=0
        ).astype(bf16)
        twice = jnp.concatenate([r.dd[j], r.dd[j]], axis=0)
        dense = dense + dot(both, twice)
    dense = mix * dense
    arrived(r.zr.at[pl.ds(0, NZ - 1)], r.zrs)
    for j in range(NZ):
        r.zf[j * zrows : (j + 1) * zrows] = r.zr[lax.rem(z - j - 1 + 2 * NZ, NZ)].astype(f32)
    results = r.zf[...].astype(bf16)
    mixed = dot(spread_high, results) + dot(spread_low, results) + dense
    for i in range(nxc * ny):
        r.cs[i] = mixed[i * rows4 : (i + 1) * rows4].astype(bf16)

    for i, (dt, dx, dc) in enumerate(plane):
        here = (cp(dc) * NX + xp(dx)) * ny + yp(dt)
        go(
            "s_out",
            r.cs.at[here],
            r.cr.at[i + 1],
            r.crs,
            ep=ep_at(z, xp(dx), cp(dc)),
            tp=yp(dt),
        )
    r.cr[0] = r.cs[(c * NX + x) * ny + t]
    res = r.resid[t]
    arrived(r.cr.at[pl.ds(1, len(plane))], r.crs)
    for j in range(ny):
        cols = slice(j * fq, (j + 1) * fq)
        moved = r.cr[pl.ds(yp(-j) * nxc, nxc)].astype(f32)
        r.out[:, cols] = (res[:, cols] + jnp.sum(moved, axis=0)).astype(bf16)
    sizes = dict(
        s_dd=r.dd,
        s_part=r.part,
        s_x=h_all,
        s_ring=h_all,
        s_core=h_all,
        s_tpcore=None,
        s_tp=None,
        s_act=r.asend,
        s_z=r.zs,
        s_out=r.cr,
    )
    for key, count in sent.items():
        if key == "s_y":
            whole = r.ysend
        elif key == "s_tp":
            whole = r.h_tp.at[others, pl.ds(0, NX * NZ)]
        elif key == "s_tpcore":
            whole = r.h_tp.at[others, pl.ds(0, NX * count)]
        else:
            whole = sizes[key].at[pl.ds(0, count)]
        remote(whole, whole, getattr(r, key), r.crs, ep=ep, tp=t).wait_send()


def on_device(
    tokens,
    norm1_gain,
    query_weight,
    key_weight,
    value_weight,
    forget_weight,
    forget_bias,
    out_weight,
    kv_cache,
    log_gates,
    lengths,
    norm2_gain,
    routing,
    route_weight,
    expert_gate,
    expert_up,
    expert_down,
    dense_gate,
    dense_up,
    dense_down,
    dense_mix,
):
    seq, d_model = tokens.shape
    top = routing.shape[1]
    ny = lax.axis_size("tp")
    rows4 = seq // ny
    ff = expert_gate.shape[2]
    units = dense_gate.shape[1]
    fq = d_model // ny
    nxc = NX * NC
    nblk = NC * NZ * NX
    zrows = CAP * nxc
    slots = NZ * zrows
    width = d_model // 2 + META + fq // 2
    last = NZ // 2
    f32, bf16 = jnp.float32, jnp.bfloat16
    hd2 = kv_cache.shape[3]
    vm = pltpu.VMEM

    def dma(*shape):
        return pltpu.SemaphoreType.DMA(shape) if shape else pltpu.SemaphoreType.DMA

    scratch = dict(
        h_all=vm((nblk, seq, width), bf16),
        h_tp=vm((ny, nblk, seq, fq // 2), bf16),
        hid=vm((ny, seq, fq // 2), bf16),
        kvbuf=vm((seq, kv_cache.shape[1], hd2), bf16),
        wkv=vm((hd2, d_model), bf16),
        wo=vm((hd2, d_model), bf16),
        att=vm((2 * seq, hd2), f32),
        part=vm((ny, seq, d_model), bf16),
        resid=vm((ny, rows4, d_model), f32),
        eg=vm((d_model, ff), bf16),
        eu=vm((d_model, ff), bf16),
        ed=vm((ff, d_model), bf16),
        wgu=vm((2 * units, d_model), bf16),
        dd=vm((NZ, units, fq), bf16),
        xs=vm((slots, d_model), f32),
        ysend=vm((ny - 1, NZ, zrows, fq), bf16),
        yrecv=vm((NZ, ny - 1, zrows, fq), bf16),
        rown=vm((NZ, zrows, fq), f32),
        zs=vm((NZ - 1, zrows, fq), bf16),
        zr=vm((NZ, zrows, fq), bf16),
        zf=vm((slots, fq), f32),
        asend=vm((NZ - 1, NX * seq, 2 * units), bf16),
        arecv=vm((NZ, NX * seq, 2 * units), bf16),
        cs=vm((nxc * ny, rows4, fq), bf16),
        cr=vm((nxc * ny, rows4, fq), bf16),
        wq=vm((d_model, hd2), bf16),
        qsem=dma(3),
        kvsem=dma(4),
        ldsem=dma(7),
        s1r=dma(),
        xrs=dma(max(NX - 1, 1)),
        rrs=dma(last, NX),
        lrs=dma(last, NX),
        dcr=dma(NZ),
        tpr=dma(NZ),
        dtr=dma(NZ),
        ddr=dma(),
        yrs=dma(NZ),
        zrs=dma(),
        ars=dma(),
        crs=dma(),
        s_dd=dma(),
        s_part=dma(),
        s_x=dma(),
        s_ring=dma(),
        s_core=dma(),
        s_tp=dma(),
        s_tpcore=dma(),
        s_act=dma(),
        s_y=dma(),
        s_z=dma(),
        s_out=dma(),
    )
    in_vmem = pl.BlockSpec(memory_space=pltpu.VMEM)
    in_smem = pl.BlockSpec(memory_space=pltpu.SMEM)
    in_hbm = pl.BlockSpec(memory_space=pl.ANY)
    places = [in_vmem] * VMEM_INPUTS + [in_hbm] * (len(IN_NAMES) - VMEM_INPUTS)
    places[IN_NAMES.index("lengths")] = in_smem
    places[IN_NAMES.index("fbias")] = in_smem
    names = tuple(IN_NAMES) + ("out",) + tuple(scratch)
    return pl.pallas_call(
        functools.partial(layer_kernel, names, top),
        out_shape=jax.ShapeDtypeStruct((rows4, d_model), bf16),
        in_specs=places,
        out_specs=in_vmem,
        scratch_shapes=list(scratch.values()),
        compiler_params=pltpu.CompilerParams(
            collective_id=0, has_side_effects=True, vmem_limit_bytes=60 * 1024 * 1024
        ),
        name="layer",
    )(
        tokens,
        norm1_gain.reshape(1, d_model),
        norm2_gain.reshape(1, d_model),
        dense_mix.reshape(1, d_model),
        forget_weight.T,
        forget_bias.reshape(1, -1),
        lengths,
        log_gates,
        routing.T,
        route_weight.T,
        out_weight,
        kv_cache.reshape(seq, kv_cache.shape[1], hd2),
        query_weight,
        key_weight.T,
        value_weight.T,
        expert_gate[0],
        expert_up[0],
        expert_down[0],
        dense_gate.T,
        dense_up.T,
        dense_down,
    )


def solution(mesh):
    return jax.shard_map(
        on_device,
        mesh=mesh,
        in_specs=(
            P("ep", None),
            P(),
            P(None, "tp"),
            P(None, "tp"),
            P(None, "tp"),
            P(None, "tp"),
            P("tp"),
            P("tp", None),
            P("ep", None, "tp", None),
            P("ep", "tp", None),
            P("ep"),
            P(),
            P("ep", None),
            P("ep", None),
            P("ep", None, "tp"),
            P("ep", None, "tp"),
            P("ep", "tp", None),
            P(None, "ep"),
            P(None, "ep"),
            P("ep", None),
            P(),
        ),
        out_specs=P(("ep", "tp"), None),
        check_vma=False,
    )
```

```python
import functools

import jax
import jax.numpy as jnp
from jax import lax
from jax.experimental import pallas as pl
from jax.experimental.pallas import tpu as pltpu
from jax.sharding import PartitionSpec as P

EPS = 1e-05
LIMIT = 7.0
ALPHA = 1.702
NZ, NX, NC = 8, 4, 2
CAP = 3
META = 128
MESH = pl.DeviceIdType.MESH


def clamped_unit(gate_pre, up_pre):
    capped = jnp.minimum(gate_pre, LIMIT)
    return capped * jax.nn.sigmoid(ALPHA * capped) * (jnp.clip(up_pre, -LIMIT, LIMIT) + 1.0)


def rms_scaled(values, gain_vec):
    return values * lax.rsqrt(jnp.mean(values * values, axis=-1, keepdims=True) + EPS) * gain_vec


def remote(src, dst, send_sem, recv_sem, **device):
    return pltpu.make_async_remote_copy(
        src_ref=src,
        dst_ref=dst,
        send_sem=send_sem,
        recv_sem=recv_sem,
        device_id=device,
        device_id_type=MESH,
    )


IN_NAMES = (
    "tok",
    "gain1",
    "gain2",
    "dmix",
    "fwt",
    "fbias",
    "lengths",
    "gates",
    "routing",
    "weight",
    "wout",
    "kv",
    "wq_hbm",
    "wkt",
    "wvt",
    "eg_hbm",
    "eu_hbm",
    "ed_hbm",
    "dgt",
    "dut",
    "dd_hbm",
)
VMEM_INPUTS = 10


class Refs:
    pass


def layer_kernel(names, top, *refs):
    r = Refs()
    for name, ref in zip(names, refs, strict=True):
        setattr(r, name, ref)
    seq, d_model = r.tok.shape
    ny = r.part.shape[0]
    rows4 = seq // ny
    nblk = NC * NZ * NX
    fq = d_model // ny
    nxc = NX * NC
    zrows = CAP * nxc
    slots = NZ * zrows
    per_z = NX * seq
    both_z = NC * per_z
    f32, bf16 = jnp.float32, jnp.bfloat16
    h_all = r.h_all
    ep = lax.axis_index("ep")
    t = lax.axis_index("tp")
    z = ep // nxc
    x = (ep // NC) % NX
    c = ep % NC

    def ep_at(zi, xi, ci):
        return (zi * NX + xi) * NC + ci

    def blk(ci, zi, xi):
        return (ci * NZ + zi) * NX + xi

    def yp(d):
        return lax.rem(t + d + ny, ny)

    def zp(d):
        return lax.rem(z + d + NZ, NZ)

    def xp(d):
        return lax.rem(x + d + NX, NX)

    def cp(d):
        return lax.rem(c + d, NC)

    def iota(shape, dim):
        return lax.broadcasted_iota(jnp.int32, shape, dim)

    def dot_nt(a, b):
        return lax.dot_general(a, b, (((1,), (1,)), ((), ())), preferred_element_type=f32)

    def dot(a, b):
        return jnp.dot(a, b, preferred_element_type=f32)

    y_order = sorted(range(1, ny), key=lambda d: -min(d, ny - d))

    hd = r.wkt.shape[0]
    early = [
        pltpu.make_async_copy(r.wq_hbm, r.wq, r.qsem.at[0]),
        pltpu.make_async_copy(r.wkt, r.wkv.at[pl.ds(0, hd)], r.qsem.at[1]),
        pltpu.make_async_copy(r.wvt, r.wkv.at[pl.ds(hd, hd)], r.qsem.at[2]),
    ]
    for load in early:
        load.start()
    barrier = pltpu.get_barrier_semaphore()
    plane = [(dt, dx, dc) for dt in range(ny) for dc in range(NC) for dx in range(NX)][1:]
    for dt, dx, dc in plane:
        pl.semaphore_signal(
            barrier,
            inc=1,
            device_id={"ep": ep_at(z, xp(dx), cp(dc)), "tp": yp(dt)},
            device_id_type=MESH,
        )
    for d in range(1, NZ):
        pl.semaphore_signal(
            barrier, inc=1, device_id={"ep": ep_at(zp(d), x, c)}, device_id_type=MESH
        )

    units = r.dgt.shape[0]
    kv_groups = 4
    per_group = seq // kv_groups
    kv_loads = [
        pltpu.make_async_copy(
            r.kv.at[pl.ds(i * per_group, per_group)],
            r.kvbuf.at[pl.ds(i * per_group, per_group)],
            r.kvsem.at[i],
        )
        for i in range(kv_groups)
    ]
    late = [
        (r.dd_hbm.at[:, pl.ds(pl.multiple_of(t * fq, fq), fq)], r.dd.at[NZ - 1]),
        (r.wout, r.wo),
        (r.dgt, r.wgu.at[pl.ds(0, units)]),
        (r.dut, r.wgu.at[pl.ds(units, units)]),
        (r.eg_hbm, r.eg),
        (r.eu_hbm, r.eu),
        (r.ed_hbm, r.ed),
    ]
    late = [pltpu.make_async_copy(src, dst, r.ldsem.at[i]) for i, (src, dst) in enumerate(late)]
    for load in kv_loads + late:
        load.start()

    sent = {}

    def go(key, src, dst, recv_sem, **device):
        remote(src, dst, getattr(r, key), recv_sem, **device).start()
        sent[key] = sent.get(key, 0) + 1

    def arrived(ref, recv_sem):
        remote(ref, ref, r.s_dd, recv_sem, ep=ep, tp=t).wait_recv()

    tok = r.tok[...].astype(f32)
    normed = rms_scaled(tok, r.gain1[...])
    normed = normed.astype(bf16)
    for load in early:
        load.wait()
    cache_len = r.kv.shape[1]
    scale = hd ** (-0.5)
    q = dot(normed, r.wq[...]).astype(bf16).astype(f32)
    kv_new = dot_nt(normed, r.wkv[...]).astype(bf16).astype(f32)
    low_lanes = iota((seq, 2 * hd), 1) < hd
    q_heads = [jnp.where(low_lanes, q, 0.0), jnp.where(low_lanes, pltpu.roll(q, hd, 1), 0.0)]
    wide = normed.astype(f32)
    pairs = 2 * seq
    of_pair = iota((pairs, seq), 0) == 2 * iota((pairs, seq), 1)
    of_pair1 = iota((pairs, seq), 0) == 2 * iota((pairs, seq), 1) + 1
    eye = jnp.where(iota((seq, seq), 0) == iota((seq, seq), 1), 1.0, 0.0)

    def to_pairs(first, second):
        rows = [jnp.sum(eye * v, axis=0, keepdims=True) for v in (first, second)]
        return jnp.sum(
            jnp.where(of_pair, rows[0], jnp.where(of_pair1, rows[1], 0.0)), axis=1, keepdims=True
        )

    of_heads = [jnp.where(m, 1.0, 0.0).astype(bf16) for m in (of_pair, of_pair1)]
    q_pairs = sum(dot(of_heads[h], q_heads[h].astype(bf16)) for h in range(2))
    kv_pairs = dot(of_heads[0] + of_heads[1], kv_new.astype(bf16))
    gate_new, own_exp = [], []
    for h in range(2):
        pre = jnp.sum(wide * r.fwt[h : h + 1, :].astype(f32), axis=-1, keepdims=True)
        pre = pre + r.fbias[0, h]
        gate_new.append(jnp.minimum(pre, 0.0) - jnp.log(1.0 + jnp.exp(-jnp.abs(pre))))
        own_exp.append(jnp.exp(jnp.sum(q_heads[h] * kv_new, axis=-1, keepdims=True) * scale))
    gate_new = to_pairs(*gate_new)
    own_exp = to_pairs(*own_exp)

    rt = r.routing[...].astype(f32)
    wt = r.weight[...]
    earlier = iota((seq, seq), 1) < iota((seq, seq), 0)
    lane = iota((seq, META), 1)
    meta = jnp.zeros((seq, META), f32)

    def column(row):
        return jnp.sum(eye * row, axis=-1, keepdims=True)

    for k in range(top):
        chosen = column(rt[k : k + 1])
        same = jnp.zeros((seq, seq), f32)
        for other in range(top):
            same = same + jnp.where((chosen == rt[other : other + 1]) & earlier, 1.0, 0.0)
        rank = jnp.sum(same, axis=-1, keepdims=True)
        value = column(wt[k : k + 1])
        high = value.astype(bf16).astype(f32)
        mid = (value - high).astype(bf16).astype(f32)
        parts = (4.0 * chosen + rank, high, mid, value - high - mid)
        for i, v in enumerate(parts):
            meta = jnp.where(lane == i * top + k, v, meta)

    position = iota((8, cache_len), 1)
    row_pair = iota((8, 1), 0) // 2
    row_pair_wide = iota((8, 2 * hd), 0) // 2

    for g in range(kv_groups):
        kv_loads[g].wait()
        if g == 0:
            pl.semaphore_wait(barrier, len(plane) + (NZ - 1))
            late[0].wait()
            for d in range(1, NZ):
                go("s_dd", r.dd.at[NZ - 1], r.dd.at[d - 1], r.ddr, ep=ep_at(zp(d), x, c))
        at = slice(8 * g, 8 * g + 8)
        queries = q_pairs[at]
        scores = jnp.zeros((8, cache_len), f32)
        length = jnp.zeros((8, 1), jnp.int32)
        for i in range(4):
            only = jnp.where(row_pair_wide == i, queries, 0.0).astype(bf16)
            scores = scores + dot_nt(only, r.kvbuf[4 * g + i])
            length = jnp.where(row_pair == i, r.lengths[4 * g + i], length)
        gates = jnp.concatenate([r.gates[4 * g + i] for i in range(4)], axis=0)
        last_gate = jnp.sum(
            jnp.where(position == length - 1, gates, 0.0), axis=-1, keepdims=True
        )
        bias = last_gate - gates + gate_new[at]
        cached = jnp.where(position < length, jnp.exp(scores * scale + bias), 0.0)
        whole = jnp.sum(cached, axis=-1, keepdims=True) + own_exp[at]
        probs = (cached / whole).astype(bf16)
        got = (own_exp[at] / whole).astype(bf16).astype(f32) * kv_pairs[at]
        for i in range(4):
            got = got + jnp.where(row_pair_wide == i, dot(probs, r.kvbuf[4 * g + i]), 0.0)
        r.att[at] = got
    attended = jnp.where(
        low_lanes,
        pltpu.roll(r.att[pl.ds(0, seq, stride=2)], hd, 1),
        r.att[pl.ds(1, seq, stride=2)],
    ).astype(bf16)
    late[1].wait()

    r.part[ny - 1] = dot(attended, r.wo[...]).astype(bf16)
    for d in y_order:
        go("s_part", r.part.at[ny - 1], r.part.at[d - 1], r.s1r, tp=yp(d))
    arrived(r.part.at[pl.ds(0, ny - 1)], r.s1r)
    total = jnp.zeros((seq, d_model), f32)
    for j in range(ny):
        total = total + r.part[yp(-j - 1)].astype(f32)
    res = r.tok[...].astype(f32) + total.astype(bf16).astype(f32)
    for j in range(ny):
        r.resid[j] = res[j * rows4 : (j + 1) * rows4]
    mine = h_all.at[blk(c, z, x)]
    hidden = rms_scaled(res, r.gain2[...]).astype(bf16)
    common = d_model // 2
    lanes_tp = fq // 2
    wide_at = common + META
    mine[:, :common] = hidden[:, :common]
    mine[:, common:wide_at] = meta.astype(bf16)
    for j in range(ny):
        r.hid[j] = hidden[:, common + j * lanes_tp : common + (j + 1) * lanes_tp]
    mine[:, wide_at:] = r.hid[t]

    for d in range(1, NX):
        go("s_x", mine, mine, r.xrs.at[d - 1], ep=ep_at(z, xp(d), c))

    half = (NX + 1) // 2
    last = NZ // 2

    def takes(direction, step, q):
        if step < last:
            return True
        return q < half if direction > 0 else q >= half

    def pass_on(direction, step, q):
        if step > last or not takes(direction, step, q):
            return
        block = h_all.at[blk(c, zp(-direction * (step - 1)), xp(-q))]
        rs = r.rrs if direction > 0 else r.lrs
        go("s_ring", block, block, rs.at[step - 1, q], ep=ep_at(zp(direction), x, c))

    def across(rel, q):
        block = h_all.at[blk(c, zp(rel), xp(-q))]
        go("s_core", block, block, r.dcr.at[rel % NZ], ep=ep_at(z, x, cp(1)))

    others = pl.ds(1, ny - 1)

    def row_at(ci, rel):
        return pl.ds(blk(ci, zp(rel), 0), NX)

    def give_tp(rel):
        here = h_all.at[row_at(c, rel), :, pl.ds(wide_at, lanes_tp)]
        for d in y_order:
            go("s_tp", here, r.h_tp.at[d, row_at(c, rel)], r.tpr.at[rel % NZ], tp=yp(d))

    def take_tp(rel):
        there = r.h_tp.at[others, row_at(c, rel)]
        arrived(there, r.tpr.at[rel % NZ])
        go("s_tpcore", there, there, r.dtr.at[rel % NZ], ep=ep_at(z, x, cp(1)))

    def from_other_core(rel):
        arrived(h_all.at[row_at(cp(1), rel)], r.dcr.at[rel % NZ])
        arrived(r.h_tp.at[others, row_at(cp(1), rel)], r.dtr.at[rel % NZ])
        for ci in range(NC):
            at = pl.ds(blk(ci, zp(rel), 0), NX)
            r.h_tp[0, at] = h_all[at, :, wide_at:]

    def z_step(step):
        for q in range(NX):
            for direction in (1, -1):
                if not takes(direction, step, q):
                    continue
                rs = r.rrs if direction > 0 else r.lrs
                arrived(h_all.at[blk(c, zp(-direction * step), xp(-q))], rs.at[step - 1, q])
                pass_on(direction, step + 1, q)
                across(-direction * step, q)

    def features_of(zi):
        rows = []
        for ci in range(NC):
            at = pl.ds(blk(ci, zi, 0), NX)
            parts = [h_all[at, :, :common]] + [r.h_tp[yp(-j), at] for j in range(ny)]
            rows.append(jnp.concatenate(parts, axis=-1).reshape(per_z, d_model))
        return jnp.concatenate(rows, axis=0)

    def codes_of(zi):
        parts = [h_all[pl.ds(blk(ci, zi, 0), NX), :, common:wide_at] for ci in range(NC)]
        return jnp.concatenate([v.reshape(per_z, META) for v in parts], axis=0)

    in_first = iota((per_z, 2 * units), 1) < units

    def dense_units(rel):
        zi = zp(rel)
        pre = dot_nt(features_of(zi), r.wgu[...])
        low, high = pre[:per_z], pre[per_z:]
        act = clamped_unit(
            jnp.where(in_first, low, pltpu.roll(high, units, 1)),
            jnp.where(in_first, pltpu.roll(low, units, 1), high),
        ).astype(bf16)
        d = rel % NZ
        if d == 0:
            r.arecv[NZ - 1] = act
            return
        r.asend[d - 1] = act
        go("s_act", r.asend.at[d - 1], r.arecv.at[d - 1], r.ars, ep=ep_at(zi, x, c))

    lead8 = jnp.where(iota((8, META), 0) == iota((8, META), 1), 1.0, 0.0).astype(bf16)
    code_base = (ep * 4).astype(f32)

    def pick_rows(rel):
        zi = zp(rel)
        codes = dot_nt(lead8, codes_of(zi))
        block = iota((1, both_z), 1) // seq
        where = ((block % NX) * NC + block // NX).astype(f32)
        target = jnp.full((1, both_z), -1.0, f32)
        for k in range(top):
            j = codes[k : k + 1] - code_base
            target = jnp.where((j >= 0.0) & (j <= CAP - 1.0), where + j * nxc, target)
        slot = iota((zrows, both_z), 0).astype(f32)
        return dot(jnp.where(slot == target, 1.0, 0.0).astype(bf16), features_of(zi))

    def experts_of(rels, send=True):
        start = min(i for i, rel in enumerate(z_order) if rel in rels) * zrows
        rows = len(rels) * zrows
        for i, rel in enumerate(rels):
            r.xs[start + i * zrows : start + (i + 1) * zrows] = pick_rows(rel)
        xs = r.xs[start : start + rows].astype(bf16)
        act = clamped_unit(dot(xs, r.eg[...]), dot(xs, r.eu[...])).astype(bf16)
        for d in y_order + [0]:
            peer = yp(d)
            made = dot(act, r.ed[:, pl.ds(pl.multiple_of(peer * fq, fq), fq)])
            for i, rel in enumerate(rels):
                piece = made[i * zrows : (i + 1) * zrows]
                if d == 0:
                    r.rown[rel % NZ] = piece
                    continue
                r.ysend[d - 1, rel % NZ] = piece.astype(bf16)
            if d and send:
                send_results(rels, d)

    def send_results(rels, d):
        for rel in rels:
            i = rel % NZ
            go("s_y", r.ysend.at[d - 1, i], r.yrecv.at[i, d - 1], r.yrs.at[i], tp=yp(d))

    def finish(rels):
        for rel in rels:
            d = rel % NZ
            arrived(r.yrecv.at[d], r.yrs.at[d])
            summed = r.rown[d]
            for i in range(ny - 1):
                summed = summed + r.yrecv[d, i].astype(f32)
            if d == 0:
                r.zr[NZ - 1] = summed.astype(bf16)
                continue
            r.zs[d - 1] = summed.astype(bf16)
            go("s_z", r.zs.at[d - 1], r.zr.at[d - 1], r.zrs, ep=ep_at(zp(d), x, c))

    z_order = [0]
    for step in range(1, last):
        z_order += [-step, step]
    z_order.append(last)

    for q in range(NX):
        if q:
            arrived(h_all.at[blk(c, z, xp(-q))], r.xrs.at[q - 1])
        pass_on(1, 1, q)
        pass_on(-1, 1, q)
        across(0, q)
    give_tp(0)
    for load in late[2:]:
        load.wait()
    z_step(1)
    give_tp(-1)
    if last > 1:
        give_tp(1)
    take_tp(0)

    parts = [[0, -1, 1], [-2, 2], [4, -3, 3]] if NZ == 8 else [z_order]
    for step in range(2, last + 1):
        z_step(step)
        give_tp(-step)
        if step < last:
            give_tp(step)
        take_tp(1 - step)
        take_tp(step - 1)
        if NZ != 8:
            continue
        if step == 4:
            for d in y_order:
                send_results(parts[0], d)
        if step == 2:
            from_other_core(0)
            dense_units(0)
        elif step == 3:
            from_other_core(-1)
            from_other_core(1)
            dense_units(-1)
            dense_units(1)
            experts_of(parts[0], send=False)
        else:
            from_other_core(-2)
            from_other_core(2)
            experts_of(parts[1])
            dense_units(-2)
            dense_units(2)
    own_meta = codes_of(z).astype(f32)
    mix = jnp.sum(features_of(z).astype(f32) * r.dmix[...], axis=-1, keepdims=True)
    mix = jax.nn.sigmoid(mix)
    col = iota((1, slots), 1)
    col_block = col // nxc
    col_z = (col_block * 43) // 128
    targets = 4 * (col_z * nxc + x * NC + c) + (col_block - CAP * col_z)
    targets = targets.astype(f32)
    row_block = iota((both_z, 1), 0) // seq
    row_xc = (row_block % NX) * NC + row_block // NX
    spread = jnp.zeros((both_z, slots), f32)
    for k in range(top):
        weight = (
            own_meta[:, top + k : top + k + 1]
            + own_meta[:, 2 * top + k : 2 * top + k + 1]
            + own_meta[:, 3 * top + k : 3 * top + k + 1]
        )
        spread = spread + jnp.where(own_meta[:, k : k + 1] == targets, weight, 0.0)
    spread = jnp.where(row_xc == col % nxc, spread, 0.0)
    spread_high = spread.astype(bf16)
    spread_low = (spread - spread_high.astype(f32)).astype(bf16)

    take_tp(last)
    for rel in parts[-1]:
        from_other_core(rel)
    experts_of(parts[-1])
    for part in parts[:-1]:
        finish(part)
    for rel in reversed(z_order[5:] if NZ == 8 else z_order):
        dense_units(rel)

    finish(parts[-1])

    arrived(r.dd.at[pl.ds(0, NZ - 1)], r.ddr)
    arrived(r.arecv.at[pl.ds(0, NZ - 1)], r.ars)
    dense = jnp.zeros((both_z, fq), f32)
    for j in range(NZ):
        got = r.arecv[j].astype(f32)
        both = jnp.concatenate(
            [jnp.where(in_first, got, 0.0), jnp.where(in_first, 0.0, got)], axis=0
        ).astype(bf16)
        twice = jnp.concatenate([r.dd[j], r.dd[j]], axis=0)
        dense = dense + dot(both, twice)
    dense = mix * dense
    arrived(r.zr.at[pl.ds(0, NZ - 1)], r.zrs)
    for j in range(NZ):
        r.zf[j * zrows : (j + 1) * zrows] = r.zr[lax.rem(z - j - 1 + 2 * NZ, NZ)].astype(f32)
    results = r.zf[...].astype(bf16)
    mixed = dot(spread_high, results) + dot(spread_low, results) + dense
    for i in range(nxc * ny):
        r.cs[i] = mixed[i * rows4 : (i + 1) * rows4].astype(bf16)

    far_first = sorted(
        enumerate(plane), key=lambda p: -(min(p[1][0], ny - p[1][0]) + min(p[1][1], NX - p[1][1]))
    )
    for i, (dt, dx, dc) in far_first:
        here = (cp(dc) * NX + xp(dx)) * ny + yp(dt)
        go(
            "s_out",
            r.cs.at[here],
            r.cr.at[i + 1],
            r.crs,
            ep=ep_at(z, xp(dx), cp(dc)),
            tp=yp(dt),
        )
    r.cr[0] = r.cs[(c * NX + x) * ny + t]
    res = r.resid[t]
    arrived(r.cr.at[pl.ds(1, len(plane))], r.crs)
    for j in range(ny):
        cols = slice(j * fq, (j + 1) * fq)
        moved = r.cr[pl.ds(yp(-j) * nxc, nxc)].astype(f32)
        r.out[:, cols] = (res[:, cols] + jnp.sum(moved, axis=0)).astype(bf16)
    sizes = dict(
        s_dd=r.dd,
        s_part=r.part,
        s_x=h_all,
        s_ring=h_all,
        s_core=h_all,
        s_tpcore=None,
        s_tp=None,
        s_act=r.asend,
        s_z=r.zs,
        s_out=r.cr,
    )
    for key, count in sent.items():
        if key == "s_y":
            whole = r.ysend
        elif key == "s_tp":
            whole = r.h_tp.at[others, pl.ds(0, NX * NZ)]
        elif key == "s_tpcore":
            whole = r.h_tp.at[others, pl.ds(0, NX * count)]
        else:
            whole = sizes[key].at[pl.ds(0, count)]
        remote(whole, whole, getattr(r, key), r.crs, ep=ep, tp=t).wait_send()


def on_device(
    tokens,
    norm1_gain,
    query_weight,
    key_weight,
    value_weight,
    forget_weight,
    forget_bias,
    out_weight,
    kv_cache,
    log_gates,
    lengths,
    norm2_gain,
    routing,
    route_weight,
    expert_gate,
    expert_up,
    expert_down,
    dense_gate,
    dense_up,
    dense_down,
    dense_mix,
):
    seq, d_model = tokens.shape
    top = routing.shape[1]
    ny = lax.axis_size("tp")
    rows4 = seq // ny
    ff = expert_gate.shape[2]
    units = dense_gate.shape[1]
    fq = d_model // ny
    nxc = NX * NC
    nblk = NC * NZ * NX
    zrows = CAP * nxc
    slots = NZ * zrows
    width = d_model // 2 + META + fq // 2
    last = NZ // 2
    f32, bf16 = jnp.float32, jnp.bfloat16
    hd2 = kv_cache.shape[3]
    vm = pltpu.VMEM

    def dma(*shape):
        return pltpu.SemaphoreType.DMA(shape) if shape else pltpu.SemaphoreType.DMA

    scratch = dict(
        h_all=vm((nblk, seq, width), bf16),
        h_tp=vm((ny, nblk, seq, fq // 2), bf16),
        hid=vm((ny, seq, fq // 2), bf16),
        kvbuf=vm((seq, kv_cache.shape[1], hd2), bf16),
        wkv=vm((hd2, d_model), bf16),
        wo=vm((hd2, d_model), bf16),
        att=vm((2 * seq, hd2), f32),
        part=vm((ny, seq, d_model), bf16),
        resid=vm((ny, rows4, d_model), f32),
        eg=vm((d_model, ff), bf16),
        eu=vm((d_model, ff), bf16),
        ed=vm((ff, d_model), bf16),
        wgu=vm((2 * units, d_model), bf16),
        dd=vm((NZ, units, fq), bf16),
        xs=vm((slots, d_model), f32),
        ysend=vm((ny - 1, NZ, zrows, fq), bf16),
        yrecv=vm((NZ, ny - 1, zrows, fq), bf16),
        rown=vm((NZ, zrows, fq), f32),
        zs=vm((NZ - 1, zrows, fq), bf16),
        zr=vm((NZ, zrows, fq), bf16),
        zf=vm((slots, fq), f32),
        asend=vm((NZ - 1, NX * seq, 2 * units), bf16),
        arecv=vm((NZ, NX * seq, 2 * units), bf16),
        cs=vm((nxc * ny, rows4, fq), bf16),
        cr=vm((nxc * ny, rows4, fq), bf16),
        wq=vm((d_model, hd2), bf16),
        qsem=dma(3),
        kvsem=dma(4),
        ldsem=dma(7),
        s1r=dma(),
        xrs=dma(max(NX - 1, 1)),
        rrs=dma(last, NX),
        lrs=dma(last, NX),
        dcr=dma(NZ),
        tpr=dma(NZ),
        dtr=dma(NZ),
        ddr=dma(),
        yrs=dma(NZ),
        zrs=dma(),
        ars=dma(),
        crs=dma(),
        s_dd=dma(),
        s_part=dma(),
        s_x=dma(),
        s_ring=dma(),
        s_core=dma(),
        s_tp=dma(),
        s_tpcore=dma(),
        s_act=dma(),
        s_y=dma(),
        s_z=dma(),
        s_out=dma(),
    )
    in_vmem = pl.BlockSpec(memory_space=pltpu.VMEM)
    in_smem = pl.BlockSpec(memory_space=pltpu.SMEM)
    in_hbm = pl.BlockSpec(memory_space=pl.ANY)
    places = [in_vmem] * VMEM_INPUTS + [in_hbm] * (len(IN_NAMES) - VMEM_INPUTS)
    places[IN_NAMES.index("lengths")] = in_smem
    places[IN_NAMES.index("fbias")] = in_smem
    names = tuple(IN_NAMES) + ("out",) + tuple(scratch)
    return pl.pallas_call(
        functools.partial(layer_kernel, names, top),
        out_shape=jax.ShapeDtypeStruct((rows4, d_model), bf16),
        in_specs=places,
        out_specs=in_vmem,
        scratch_shapes=list(scratch.values()),
        compiler_params=pltpu.CompilerParams(
            collective_id=0, has_side_effects=True, vmem_limit_bytes=60 * 1024 * 1024
        ),
        name="layer",
    )(
        tokens,
        norm1_gain.reshape(1, d_model),
        norm2_gain.reshape(1, d_model),
        dense_mix.reshape(1, d_model),
        forget_weight.T,
        forget_bias.reshape(1, -1),
        lengths,
        log_gates,
        routing.T,
        route_weight.T,
        out_weight,
        kv_cache.reshape(seq, kv_cache.shape[1], hd2),
        query_weight,
        key_weight.T,
        value_weight.T,
        expert_gate[0],
        expert_up[0],
        expert_down[0],
        dense_gate.T,
        dense_up.T,
        dense_down,
    )


def solution(mesh):
    return jax.shard_map(
        on_device,
        mesh=mesh,
        in_specs=(
            P("ep", None),
            P(),
            P(None, "tp"),
            P(None, "tp"),
            P(None, "tp"),
            P(None, "tp"),
            P("tp"),
            P("tp", None),
            P("ep", None, "tp", None),
            P("ep", "tp", None),
            P("ep"),
            P(),
            P("ep", None),
            P("ep", None),
            P("ep", None, "tp"),
            P("ep", None, "tp"),
            P("ep", "tp", None),
            P(None, "ep"),
            P(None, "ep"),
            P("ep", None),
            P(),
        ),
        out_specs=P(("ep", "tp"), None),
        check_vma=False,
    )
```
